512 devices in a mesh: ep: 128 (over z, y, core), tp: 4 (over x).
Axes of the slice: x: 4, y: 8, z: 8, core: 2. Of those that a mesh axis runs over, the one named last changes fastest.
Arguments:
- tokens: bfloat16 [256, 2048], P('ep'), may hold values from -6 to 6
- w_query: bfloat16 [2048, 512], P(None, 'tp'), may hold values from -0.125 to 0.125
- w_key: bfloat16 [2048, 512], P(None, 'tp'), may hold values from -0.125 to 0.125
- w_value: bfloat16 [2048, 512], P(None, 'tp'), may hold values from -0.125 to 0.125
- w_forget: bfloat16 [4, 2048], P('tp'), may hold values from -0.25 to 0.25
- w_output: bfloat16 [512, 2048], P('tp'), may hold values from -0.25 to 0.25
- cache_keys: bfloat16 [256, 4, 1024, 128], P('ep', 'tp'), may hold values from -1000 to 1000
- cache_values: bfloat16 [256, 4, 1024, 128], P('ep', 'tp'), may hold values from -6 to 6
- cache_gates: float32 [256, 4, 1024], P('ep', 'tp'), may hold values from -68 to 0, as said below
- lengths: int32 [256], P('ep'), may hold values from 2 to 1024, as said below
- ln1_gain: float32 [2048], replicated, may hold values from 0.4 to 6
- ln1_shift: float32 [2048], replicated, may hold values from -1.8 to 1.8
- gate_vector: bfloat16 [2048], replicated, may hold values from -0.125 to 0.125
- dense_gate: bfloat16 [2048, 8192], P(None, ('ep', 'tp')), may hold values from -0.125 to 0.125
- dense_up: bfloat16 [2048, 8192], P(None, ('ep', 'tp')), may hold values from -0.125 to 0.125
- dense_down: bfloat16 [8192, 2048], P(('ep', 'tp')), may hold values from -0.0625 to 0.0625
- expert_gate: bfloat16 [128, 2048, 512], P('ep', None, 'tp'), may hold values from -0.125 to 0.125
- expert_up: bfloat16 [128, 2048, 512], P('ep', None, 'tp'), may hold values from -0.125 to 0.125
- expert_down: bfloat16 [128, 512, 2048], P('ep', 'tp'), may hold values from -0.25 to 0.25
- expert_ids: int32 [256, 2], replicated, may hold values from 0 to 127, as said below
- expert_weights: float32 [256, 2], replicated, may hold values from 0.1 to 1
- ln2_gain: float32 [2048], P('tp'), may hold values from 0.1 to 1.9
- ln2_shift: float32 [2048], P('tp'), may hold values from -1.8 to 1.8
Outputs:
- mixed: bfloat16 [256, 2048], P('ep', 'tp')
The draws below stay inside these ranges and needn't reach their ends.
Inputs may be any that keep to these rules, and one draw needn't show every extreme that they name: `expert_ids`: each row names 2 different experts, all of them within one group of 4 consecutive expert numbers. `lengths`: some sequence has all 1024 positions in use. `cache_gates`: each head's values do not rise along positions.
All inputs are finite; a program needn't handle non-finite values.
Results may differ from the reference program's by a relative error of at most 0.012.
Values may be sent and summed in bfloat16 or wider, within the bound.
No kernel may reach another device: no remote copies, remote signals or barrier semaphores. Data moves between devices by JAX's collectives and lax.ppermute only.
A program may use at most 64 MiB of HBM per device.

```python
import math
import jax
import jax.numpy as jnp
from jax import lax

D = 2048
HEADS = 4
HD = 128
EXP_FF = 512
DENSE_FF = 8192
TOP = 2
PER_GROUP = 4
CACHE_LENGTH = 1024
TOKENS = 256
EXPERTS = 128


def draw_cache_keys(key, part):
    key_base = jax.random.fold_in(key, 0)
    base_keys = jax.random.normal(key_base, (TOKENS, HEADS, CACHE_LENGTH, HD), jnp.float32)
    return base_keys.astype(jnp.bfloat16)


def draw_cache_gates(key, part):
    subkeys = jax.random.split(key, 6)
    slow_share = 0.5
    slow_heads = jax.random.uniform(subkeys[0], (TOKENS, HEADS, 1), jnp.float32) < slow_share
    fast_rate = jnp.exp(jax.random.uniform(subkeys[1], (TOKENS, HEADS, 1), jnp.float32, math.log(1.0 / 100.0), math.log(1.0 / 30.0)))
    slow_rate = jnp.exp(jax.random.uniform(subkeys[2], (TOKENS, HEADS, 1), jnp.float32, math.log(0.2), math.log(0.8))) / CACHE_LENGTH
    decay_rates = jnp.where(slow_heads, slow_rate, fast_rate)
    noise_level = jax.random.uniform(subkeys[3], (TOKENS, HEADS, CACHE_LENGTH), jnp.float32, 0.3, 1.7)
    location_list = jax.random.randint(subkeys[4], (TOKENS, 1, 2), 0, CACHE_LENGTH)
    spike_counter = jnp.sum((jnp.arange(CACHE_LENGTH)[None, :, None] == location_list).astype(jnp.float32), axis=2)
    total_quantity = jax.random.uniform(subkeys[5], (TOKENS, HEADS, 1), jnp.float32, 0.22, 0.69)
    reduction_step = decay_rates * noise_level + spike_counter[:, None, :] * total_quantity
    return -jnp.cumsum(reduction_step, axis=2)


def draw_lengths(key, part):
    key_len, key_full = jax.random.split(key)
    drawn = jax.random.randint(key_len, (TOKENS,), 2, CACHE_LENGTH + 1)
    chosen = jax.random.randint(key_full, (), 0, TOKENS)
    return jnp.where(jnp.arange(TOKENS) == chosen, CACHE_LENGTH, drawn).astype(jnp.int32)


def draw_ln1_gain(key, part):
    positions = jnp.arange(D, dtype=jnp.float32) / D
    slope = math.log(3.0)
    jitter = jax.random.uniform(key, (D,), jnp.float32, 0.82, 1.18)
    return 0.5 * jnp.exp(slope * positions) * jitter


def draw_expert_ids(key, part):
    key_group, key_rank = jax.random.split(key)
    groups = jax.random.randint(key_group, (TOKENS, 1), 0, EXPERTS // PER_GROUP)
    scores = jax.random.randint(key_rank, (TOKENS, PER_GROUP), 0, 1 << 20) * PER_GROUP + jnp.arange(PER_GROUP)[None, :]
    ranking = jnp.argsort(scores, axis=1)
    return (groups * PER_GROUP + ranking[:, :TOP]).astype(jnp.int32)


def block_levels(key, extent, pieces, least, top_value):
    loudness, own = 1.0, jax.random.fold_in(key, 6)
    for dim, parts in pieces:
        steps = jnp.exp(jax.random.uniform(jax.random.fold_in(own, dim), (parts,), jnp.float32, least / len(pieces), top_value / len(pieces)))
        loudness = loudness * jnp.repeat(steps, extent[dim] // parts).reshape([-1 if axis == dim else 1 for axis in range(len(extent))])
    return loudness


def normal_values(own_key, extent, deviation, limit, pieces=(), kind=jnp.bfloat16):
    factor_of = block_levels(own_key, extent, pieces, -0.22, 0.18) if pieces else 1.0
    entries = jax.random.normal(own_key, extent, jnp.float32) * deviation * factor_of
    return jnp.minimum(jnp.maximum(entries, -limit), limit).astype(kind)


def setup_inputs(seed: int = 0) -> dict:
    key_of = jax.random.split(jax.random.key(seed), 24)
    tokens = normal_values(key_of[0], (TOKENS, D), 1.0, 6.0, ((0, 128),))
    w_query = normal_values(key_of[1], (D, HEADS * HD), D ** -0.5, 0.125, ((1, 4),))
    w_key = normal_values(key_of[2], (D, HEADS * HD), D ** -0.5, 0.125, ((1, 4),))
    w_value = normal_values(key_of[3], (D, HEADS * HD), D ** -0.5, 0.125, ((1, 4),))
    w_forget = normal_values(key_of[4], (HEADS, D), (D // 4) ** -0.5, 0.25, ((0, 4),))
    w_output = normal_values(key_of[5], (HEADS * HD, D), (HEADS * HD) ** -0.5, 0.25, ((0, 4),))
    cache_keys = draw_cache_keys(jax.random.fold_in(key_of[23], 71), 0)
    cache_values = normal_values(key_of[7], (TOKENS, HEADS, CACHE_LENGTH, HD), 1.0, 6.0, ((0, 128), (1, 4)))
    cache_gates = draw_cache_gates(jax.random.fold_in(key_of[23], 71), 0)
    lengths = draw_lengths(jax.random.fold_in(key_of[23], 71), 0)
    ln1_gain = draw_ln1_gain(jax.random.fold_in(key_of[23], 71), 0)
    ln1_shift = normal_values(key_of[11], (D,), 0.3, 1.8, (), jnp.float32)
    gate_vector = normal_values(key_of[12], (D,), D ** -0.5, 0.125)
    dense_gate = normal_values(key_of[13], (D, DENSE_FF), D ** -0.5, 0.125, ((1, 512),))
    dense_up = normal_values(key_of[14], (D, DENSE_FF), D ** -0.5, 0.125, ((1, 512),))
    dense_down = normal_values(key_of[15], (DENSE_FF, D), DENSE_FF ** -0.5, 0.0625, ((0, 512),))
    expert_gate = normal_values(key_of[16], (EXPERTS, D, EXP_FF), D ** -0.5, 0.125, ((0, 128), (2, 4)))
    expert_up = normal_values(key_of[17], (EXPERTS, D, EXP_FF), D ** -0.5, 0.125, ((0, 128), (2, 4)))
    expert_down = normal_values(key_of[18], (EXPERTS, EXP_FF, D), EXP_FF ** -0.5, 0.25, ((0, 128), (1, 4)))
    expert_ids = draw_expert_ids(jax.random.fold_in(key_of[23], 71), 0)
    expert_weights = jnp.clip(jax.random.uniform(key_of[20], (TOKENS, TOP), jnp.float32, 0.1, 1.0), 0.1, 1.0)
    ln2_gain = jnp.clip(1.0 + 0.18 * jax.random.normal(key_of[21], (D,), jnp.float32), 0.1, 1.9)
    ln2_shift = normal_values(key_of[22], (D,), 0.3, 1.8, ((0, 4),), jnp.float32)
    return dict(tokens=tokens, w_query=w_query, w_key=w_key, w_value=w_value, w_forget=w_forget, w_output=w_output, cache_keys=cache_keys, cache_values=cache_values, cache_gates=cache_gates, lengths=lengths, ln1_gain=ln1_gain, ln1_shift=ln1_shift, gate_vector=gate_vector, dense_gate=dense_gate, dense_up=dense_up, dense_down=dense_down, expert_gate=expert_gate, expert_up=expert_up, expert_down=expert_down, expert_ids=expert_ids, expert_weights=expert_weights, ln2_gain=ln2_gain, ln2_shift=ln2_shift)


alpha_scale = 1.4142135623730951
norm_eps = 1e-05

def layer_norm(values_in, gain_vec, shift_vec):
    row_mean = lax.optimization_barrier(jnp.mean(values_in, axis=-1, keepdims=True))
    row_var = lax.optimization_barrier(jnp.mean(values_in * values_in, axis=-1, keepdims=True)) - row_mean * row_mean
    return (values_in - row_mean) * lax.rsqrt(row_var + norm_eps) * gain_vec + shift_vec

def attend_one(inputs):
    query_row, key_new, value_new, forget_row, key_cache, value_cache, gate_cache, length = inputs
    score_scale = HD ** (-0.5)
    positions = jnp.arange(CACHE_LENGTH, dtype=jnp.int32)
    query_f = query_row.astype(jnp.float32)
    cache_scores = jnp.einsum('hd,hpd->hp', query_f, key_cache.astype(jnp.float32)) * score_scale
    last_gate = lax.optimization_barrier(jnp.sum(jnp.where(positions[None, :] == length - 1, gate_cache, jnp.float32(0.0)), axis=1))
    decay_bias = (last_gate + forget_row)[:, None] - gate_cache
    cache_scores = jnp.where(positions[None, :] < length, cache_scores + decay_bias, -jnp.inf)
    own_score = lax.optimization_barrier(jnp.sum(query_f * key_new.astype(jnp.float32), axis=1)) * score_scale
    all_scores = jnp.concatenate([cache_scores, own_score[:, None]], axis=1)
    probs = jax.nn.softmax(all_scores, axis=-1).astype(jnp.bfloat16)
    weighted = jnp.einsum('hp,hpd->hd', probs[:, :CACHE_LENGTH].astype(jnp.float32), value_cache.astype(jnp.float32))
    weighted = weighted + probs[:, CACHE_LENGTH:].astype(jnp.float32) * value_new.astype(jnp.float32)
    return weighted.astype(jnp.bfloat16)

def reference(tokens, w_query, w_key, w_value, w_forget, w_output, cache_keys, cache_values, cache_gates, lengths, ln1_gain, ln1_shift, gate_vector, dense_gate, dense_up, dense_down, expert_gate, expert_up, expert_down, expert_ids, expert_weights, ln2_gain, ln2_shift):
    query_rows = jnp.dot(tokens, w_query, preferred_element_type=jnp.float32).astype(jnp.bfloat16).reshape(TOKENS, HEADS, HD)
    new_keys = jnp.dot(tokens, w_key, preferred_element_type=jnp.float32).astype(jnp.bfloat16).reshape(TOKENS, HEADS, HD)
    new_values = jnp.dot(tokens, w_value, preferred_element_type=jnp.float32).astype(jnp.bfloat16).reshape(TOKENS, HEADS, HD)
    forget_new = jax.nn.log_sigmoid(jnp.dot(tokens, w_forget.T, preferred_element_type=jnp.float32))
    head_output = lax.map(attend_one, (query_rows, new_keys, new_values, forget_new, cache_keys, cache_values, cache_gates, lengths))
    attention = jnp.zeros((TOKENS, D), jnp.float32)
    for head_index in range(HEADS):
        term = jnp.dot(head_output[:, head_index], w_output[head_index * HD:(head_index + 1) * HD], preferred_element_type=jnp.float32).astype(jnp.bfloat16)
        attention = attention + term.astype(jnp.float32)
    hidden = layer_norm(alpha_scale * tokens.astype(jnp.float32) + attention, ln1_gain, ln1_shift).astype(jnp.bfloat16)
    mixing = jax.nn.sigmoid(jnp.dot(hidden, gate_vector, preferred_element_type=jnp.float32))
    dense_a = jnp.dot(hidden, dense_gate, preferred_element_type=jnp.float32)
    dense_b = jnp.dot(hidden, dense_up, preferred_element_type=jnp.float32)
    dense_hidden = (jax.nn.silu(dense_a) * dense_b * mixing[:, None]).astype(jnp.bfloat16)
    branches = jnp.dot(dense_hidden, dense_down, preferred_element_type=jnp.float32)
    expert_range = jnp.arange(EXPERTS, dtype=jnp.int32)
    route_share = lax.optimization_barrier(jnp.sum(jnp.where(expert_ids[:, :, None] == expert_range[None, None, :], expert_weights[:, :, None], jnp.float32(0.0)), axis=1))

    def one_expert(carry, inputs):
        gate_w, up_w, down_w, share_col = inputs
        part_a = jnp.dot(hidden, gate_w, preferred_element_type=jnp.float32)
        part_b = jnp.dot(hidden, up_w, preferred_element_type=jnp.float32)
        expert_hidden = (jax.nn.silu(part_a) * part_b * share_col[:, None]).astype(jnp.bfloat16)
        return (carry + jnp.dot(expert_hidden, down_w, preferred_element_type=jnp.float32), None)
    branches, _ = lax.scan(one_expert, branches, (expert_gate, expert_up, expert_down, route_share.T))
    final_rows = alpha_scale * hidden.astype(jnp.float32) + branches
    return layer_norm(final_rows, ln2_gain, ln2_shift).astype(jnp.bfloat16)
```

```python
import jax
import jax.numpy as jnp
from jax import lax
from jax.sharding import Mesh
from jax.sharding import PartitionSpec as P

EP = ("ep_0", "ep_1", "ep_2")
EP_TP = ("ep_0", "ep_1", "ep_2", "tp")


PLANE = ("ep_0", "ep_1")
OTHER_CORE = ((0, 1), (1, 0))

alpha_scale = 1.4142135623730951
norm_eps = 1e-05


def sent_to_all(array, axis):
    copies = jnp.broadcast_to(array, (lax.axis_size(axis), *array.shape))
    return lax.all_to_all(copies, axis, split_axis=0, concat_axis=0, tiled=True)


def of_everyone_2(array, axis):
    everything = sent_to_all(array, axis)
    return jnp.sum(everything.astype(jnp.float32), axis=0)


def in_blocks(array, dim, count):
    before, after = (array.shape[:dim], array.shape[dim + 1 :])
    return jnp.moveaxis(array.reshape(*before, count, -1, *after), dim, 0)


def summed_on_arrival(array, axis, dim):
    tiles = in_blocks(array, dim, lax.axis_size(axis))
    arrived = lax.all_to_all(tiles, axis, split_axis=0, concat_axis=0, tiled=True)
    return arrived.astype(jnp.float32).sum(axis=0)


def local_norm(values_in, gain_vec, shift_vec):
    row_mean = jnp.mean(values_in, axis=-1, keepdims=True)
    row_var = jnp.mean(values_in * values_in, axis=-1, keepdims=True) - row_mean * row_mean
    return (values_in - row_mean) * lax.rsqrt(row_var + norm_eps) * gain_vec + shift_vec


def branch_terms(
    rows, share, gate_vector, dense_gate, dense_up, dense_down, gate_own, up_own, down_own
):
    mixing = jax.nn.sigmoid(jnp.dot(rows, gate_vector, preferred_element_type=jnp.float32))
    dense_a = jnp.dot(rows, dense_gate, preferred_element_type=jnp.float32)
    dense_b = jnp.dot(rows, dense_up, preferred_element_type=jnp.float32)
    dense_hidden = (jax.nn.silu(dense_a) * dense_b * mixing[:, None]).astype(jnp.bfloat16)
    expert_a = jnp.dot(rows, gate_own, preferred_element_type=jnp.float32)
    expert_b = jnp.dot(rows, up_own, preferred_element_type=jnp.float32)
    expert_hidden = (jax.nn.silu(expert_a) * expert_b * share[:, None]).astype(jnp.bfloat16)
    return jnp.dot(dense_hidden, dense_down, preferred_element_type=jnp.float32) + jnp.dot(
        expert_hidden, down_own, preferred_element_type=jnp.float32
    )


def per_device(
    tokens,
    w_query,
    w_key,
    w_value,
    w_forget,
    w_output,
    cache_keys,
    cache_values,
    cache_gates,
    lengths,
    ln1_gain,
    ln1_shift,
    gate_vector,
    dense_gate,
    dense_up,
    dense_down,
    expert_gate,
    expert_up,
    expert_down,
    expert_ids,
    expert_weights,
    ln2_gain,
    ln2_shift,
):
    expert_index = lax.axis_index(EP)
    core = lax.axis_index("ep_2")
    route_share = jnp.sum(jnp.where(expert_ids == expert_index, expert_weights, 0.0), axis=1)
    by_core = route_share.reshape(-1, 2, tokens.shape[0])
    share_near = jnp.where(core == 0, by_core[:, 0], by_core[:, 1]).reshape(-1)
    share_far = jnp.where(core == 0, by_core[:, 1], by_core[:, 0]).reshape(-1)
    own_start = lax.axis_index("tp") * ln2_gain.shape[0]
    tokens, share_near, share_far, own_start = lax.optimization_barrier(
        (tokens, share_near, share_far, own_start)
    )
    query_rows = jnp.dot(tokens, w_query, preferred_element_type=jnp.float32).astype(jnp.bfloat16)
    new_keys = jnp.dot(tokens, w_key, preferred_element_type=jnp.float32).astype(jnp.bfloat16)
    new_values = jnp.dot(tokens, w_value, preferred_element_type=jnp.float32).astype(jnp.bfloat16)
    forget_new = jax.nn.log_sigmoid(
        jnp.einsum("sd,hd->sh", tokens, w_forget, preferred_element_type=jnp.float32)
    )[:, 0]
    score_scale = query_rows.shape[1] ** (-0.5)
    key_block = cache_keys[:, 0]
    value_block = cache_values[:, 0]
    gate_block = cache_gates[:, 0]
    positions = lax.broadcasted_iota(jnp.int32, gate_block.shape, 1)
    last_gate = jnp.sum(jnp.where(positions == lengths[:, None] - 1, gate_block, 0.0), axis=1)
    decay_bias = (last_gate + forget_new)[:, None] - gate_block
    scores = (
        jnp.einsum("sd,spd->sp", query_rows, key_block, preferred_element_type=jnp.float32)
        * score_scale
    )
    scores = jnp.where(positions < lengths[:, None], scores + decay_bias, -jnp.inf)
    own_score = (
        jnp.sum(query_rows.astype(jnp.float32) * new_keys.astype(jnp.float32), axis=1) * score_scale
    )
    peak = jnp.maximum(jnp.max(scores, axis=1), own_score)
    exp_terms = jnp.exp(scores - peak[:, None])
    own_exp = jnp.exp(own_score - peak)
    denominator = jnp.sum(exp_terms, axis=1) + own_exp
    probs = (exp_terms / denominator[:, None]).astype(jnp.bfloat16)
    own_prob = (own_exp / denominator).astype(jnp.bfloat16)
    weighted = jnp.einsum("sp,spd->sd", probs, value_block, preferred_element_type=jnp.float32)
    weighted = weighted + own_prob.astype(jnp.float32)[:, None] * new_values.astype(jnp.float32)
    head_output = weighted.astype(jnp.bfloat16)
    head_term = jnp.dot(head_output, w_output, preferred_element_type=jnp.float32).astype(
        jnp.bfloat16
    )
    attention = of_everyone_2(head_term, "tp").astype(jnp.float32)
    hidden = local_norm(
        alpha_scale * tokens.astype(jnp.float32) + attention, ln1_gain, ln1_shift
    ).astype(jnp.bfloat16)
    rows = sent_to_all(hidden, PLANE).reshape(-1, hidden.shape[1])
    rows_far = lax.ppermute(rows, "ep_2", OTHER_CORE)
    weights = (
        gate_vector,
        dense_gate,
        dense_up,
        dense_down,
        expert_gate[0],
        expert_up[0],
        expert_down[0],
    )
    terms_near = branch_terms(rows, share_near, *weights)
    terms_far = branch_terms(rows_far, share_far, *weights).astype(jnp.bfloat16)
    terms_here = lax.ppermute(terms_far, "ep_2", OTHER_CORE)
    terms = (terms_near + terms_here.astype(jnp.float32)).astype(jnp.bfloat16)
    owned = lax.optimization_barrier(summed_on_arrival(terms, PLANE, 0)).astype(jnp.bfloat16)
    branches = of_everyone_2(owned, "tp")
    final_rows = alpha_scale * hidden.astype(jnp.float32) + branches
    row_mean = jnp.mean(final_rows, axis=-1, keepdims=True)
    row_var = jnp.mean(final_rows * final_rows, axis=-1, keepdims=True) - row_mean * row_mean
    own_cols = ln2_gain.shape[0]
    own_rows = lax.dynamic_slice_in_dim(
        final_rows, own_start, own_cols, 1, allow_negative_indices=False
    )
    scaled = (own_rows - row_mean) * lax.rsqrt(row_var + norm_eps)
    return (scaled * ln2_gain + ln2_shift).astype(jnp.bfloat16)


def solution(mesh):
    torus = Mesh(mesh.devices.reshape(8, 8, 2, mesh.shape["tp"]), ("ep_0", "ep_1", "ep_2", "tp"))
    in_specs = (
        P(EP, None),
        P(None, "tp"),
        P(None, "tp"),
        P(None, "tp"),
        P("tp", None),
        P("tp", None),
        P(EP, "tp", None, None),
        P(EP, "tp", None, None),
        P(EP, "tp", None),
        P(EP),
        P(),
        P(),
        P(),
        P(None, EP_TP),
        P(None, EP_TP),
        P(EP_TP, None),
        P(EP, None, "tp"),
        P(EP, None, "tp"),
        P(EP, "tp", None),
        P(),
        P(),
        P("tp"),
        P("tp"),
    )
    out_specs = P(EP, "tp")
    return jax.shard_map(
        per_device, mesh=torus, in_specs=in_specs, out_specs=out_specs, check_vma=False
    )
```

```python
import functools

import jax
import jax.numpy as jnp
from jax import lax
from jax.experimental import pallas as pl
from jax.experimental.pallas import tpu as pltpu
from jax.sharding import Mesh
from jax.sharding import PartitionSpec as P

EP = ("ep_0", "ep_1", "ep_2")
EP_TP = ("ep_0", "ep_1", "ep_2", "tp")
PLANE = ("ep_0", "ep_1")
OTHER_CORE = ((0, 1), (1, 0))

alpha_scale = 1.4142135623730951
norm_eps = 1e-05

F32 = jnp.float32
BF16 = jnp.bfloat16
ANY = pl.BlockSpec(memory_space=pl.ANY)
VMEM = pl.BlockSpec(memory_space=pltpu.VMEM)
SMEM = pl.BlockSpec(memory_space=pltpu.SMEM)
NT = (((1,), (1,)), ((), ()))


def dot(a, b):
    return jnp.dot(a, b, preferred_element_type=F32)


def dot_nt(a, b):
    return lax.dot_general(a, b, NT, preferred_element_type=F32)


def in_vmem(x):
    return pltpu.with_memory_space_constraint(x, pltpu.VMEM)


def params(mib):
    return pltpu.CompilerParams(vmem_limit_bytes=mib << 20)


def attend_kernel(
    lengths_hbm,
    tokens_hbm,
    w_forget_hbm,
    cache_gates_hbm,
    w_query,
    w_key,
    w_value,
    w_output,
    cache_keys,
    cache_values,
    *rest,
):
    kept = (len(rest) - 13) // 2
    sources, (terms, tokens, *places) = rest[:kept], rest[kept : 2 * kept + 2]
    scratch = rest[2 * kept + 2 :]
    lengths, w_forget, cache_gates, q_v, k_v, v_v, o_v, keys_v, values_v, sems, kept_sems = scratch
    moves = [
        pltpu.make_async_copy(src, dst, sems.at[i])
        for i, (src, dst) in enumerate(
            (
                (tokens_hbm, tokens),
                (w_forget_hbm, w_forget),
                (lengths_hbm, lengths),
                (cache_gates_hbm, cache_gates),
                (w_query, q_v),
                (w_key, k_v),
                (cache_keys, keys_v),
                (w_value, v_v),
                (cache_values, values_v),
                (w_output, o_v),
            )
        )
    ]
    kept_moves = [
        pltpu.make_async_copy(src, dst, kept_sems.at[i])
        for i, (src, dst) in enumerate(zip(sources, places))
    ]
    for move in moves + kept_moves:
        move.start()

    for move in moves[:4]:
        move.wait()
    x = tokens[...]
    scale = w_query.shape[1] ** (-0.5)
    length = cache_gates.shape[2]
    forget = jnp.sum(x.astype(F32) * w_forget[...].astype(F32), axis=1, keepdims=True)
    forget_new = jax.nn.log_sigmoid(forget)
    second = lax.broadcasted_iota(jnp.int32, (2, 1), 0) == 1
    used = jnp.where(second, lengths[1], lengths[0])
    gates = jnp.where(second, cache_gates[1], cache_gates[0])
    positions = lax.broadcasted_iota(jnp.int32, (2, length), 1)
    last_gate = jnp.sum(jnp.where(positions == used - 1, gates, 0.0), axis=1, keepdims=True)
    decay_bias = (last_gate + forget_new) - gates

    moves[4].wait()
    query = dot(x, q_v[...]).astype(BF16)
    moves[5].wait()
    new_key = dot(x, k_v[...]).astype(BF16)
    own_score = (
        jnp.sum(query.astype(F32) * new_key.astype(F32), axis=1, keepdims=True) * scale
    )
    moves[6].wait()
    scores = jnp.where(second, dot_nt(query, keys_v[1, 0]), dot_nt(query, keys_v[0, 0])) * scale
    scores = jnp.where(positions < used, scores + decay_bias, -jnp.inf)
    peak = jnp.maximum(jnp.max(scores, axis=1, keepdims=True), own_score)
    exp_terms = jnp.exp(scores - peak)
    own_exp = jnp.exp(own_score - peak)
    denominator = jnp.sum(exp_terms, axis=1, keepdims=True) + own_exp
    probs = (exp_terms / denominator).astype(BF16)
    own_prob = (own_exp / denominator).astype(BF16)
    moves[7].wait()
    new_value = dot(x, v_v[...]).astype(BF16)
    moves[8].wait()
    weighted = jnp.where(second, dot(probs, values_v[1, 0]), dot(probs, values_v[0, 0]))
    weighted = weighted + own_prob.astype(F32) * new_value.astype(F32)
    moves[9].wait()
    term = dot(weighted.astype(BF16), o_v[...]).astype(BF16)
    for i in range(terms.shape[0]):
        terms[i] = term
    for move in kept_moves:
        move.wait()


def attend(copies, operands, kept):
    operands = [pltpu.with_memory_space_constraint(a, pltpu.HBM) for a in (*operands, *kept)]
    lengths, tokens, w_forget, gates, w_query, w_key, w_value, w_output, keys, values = operands[:10]
    held = (w_forget, gates, w_query, w_key, w_value, w_output, keys, values)
    return pl.pallas_call(
        attend_kernel,
        out_shape=[pltpu.VMEM((copies, tokens.shape[0], w_output.shape[1]), BF16)]
        + [pltpu.VMEM(a.shape, a.dtype) for a in (tokens, *kept)],
        in_specs=[pl.BlockSpec(memory_space=pltpu.HBM)] * len(operands),
        out_specs=[VMEM] * (2 + len(kept)),
        scratch_shapes=[
            pltpu.SMEM(lengths.shape, jnp.int32),
            *(pltpu.VMEM(a.shape, a.dtype) for a in held),
            pltpu.SemaphoreType.DMA((10,)),
            pltpu.SemaphoreType.DMA((len(kept),)),
        ],
        compiler_params=params(12),
        name="attend",
    )(*operands)


def normed(rows, width):
    row_mean = jnp.sum(rows, axis=-1, keepdims=True) * (1.0 / width)
    row_var = jnp.sum(rows * rows, axis=-1, keepdims=True) * (1.0 / width) - row_mean * row_mean
    return (rows - row_mean) * lax.rsqrt(row_var + norm_eps)


def hidden_kernel(heads, tokens, gain, shift, copies):
    attention = heads[0].astype(F32)
    for i in range(1, heads.shape[0]):
        attention = attention + heads[i].astype(F32)
    rows = alpha_scale * tokens[...].astype(F32) + attention
    hidden = (normed(rows, rows.shape[1]) * gain[...] + shift[...]).astype(BF16)
    for i in range(copies.shape[0]):
        copies[i] = hidden


def hidden_copies(count, heads, tokens, gain, shift):
    return pl.pallas_call(
        hidden_kernel,
        out_shape=pltpu.VMEM((count, *tokens.shape), BF16),
        in_specs=[VMEM] * 4,
        out_specs=VMEM,
        compiler_params=params(4),
        name="hidden_copies",
    )(in_vmem(heads), tokens, in_vmem(gain), in_vmem(shift))


def unit_values(far, rows, gate_vector, gate, up, dense_gate, dense_up, ids, shares):
    tokens = ids.shape[1]
    core = lax.axis_index("ep_2")
    expert = (lax.axis_index("ep_0") * lax.axis_size("ep_1") + lax.axis_index("ep_1")) * 2 + core
    side = 1 - core if far else core
    picked = jnp.where(ids[...] == expert, shares[...], 0.0)
    share_row = picked[0:1] + picked[1:2]
    count = rows.shape[0]
    row = lax.broadcasted_iota(jnp.int32, (count, tokens), 0)
    column = lax.broadcasted_iota(jnp.int32, (count, tokens), 1)
    match = column == 4 * (row >> 1) + 2 * side + (row & 1)
    share = jnp.sum(jnp.where(match, share_row, 0.0), axis=1, keepdims=True)
    x = rows[...]
    a = dot(x, gate[...])
    b = dot(x, up[...])
    units = (a / (1.0 + jnp.exp(-a)) * b * share).astype(BF16)
    dense_a = dot_nt(x, dense_gate[...])
    dense_b = dot_nt(x, dense_up[...])
    gates = jnp.broadcast_to(gate_vector[...], dense_gate.shape)
    mixing = 1.0 / (1.0 + jnp.exp(-dot_nt(x, gates)))
    dense = (dense_a / (1.0 + jnp.exp(-dense_a)) * dense_b * mixing).astype(BF16)
    return units, dense


def units_kernel(rows, gate_vector, gate, up, dense_gate, dense_up, ids, shares, units, dense):
    units[...], dense[...] = unit_values(
        False, rows, gate_vector, gate, up, dense_gate, dense_up, ids, shares
    )


def branch_kernel(
    after, rows, gate_vector, gate, up, dense_gate, dense_up, ids, shares, down, dense_down, terms
):
    units, dense = unit_values(
        True, rows, gate_vector, gate, up, dense_gate, dense_up, ids, shares
    )
    terms[...] = (dot(units, down[...]) + dot(dense, dense_down[...])).astype(BF16)


def down_kernel(units, dense, down, dense_down, terms):
    terms[...] = dot(units[...], down[...]) + dot(dense[...], dense_down[...])


def estimate(rows, depth, columns):
    return pl.CostEstimate(
        flops=2 * rows * depth * columns, bytes_accessed=4096, transcendentals=0
    )


def near_units(rows, gate_vector, gate, up, dense_gate, *rest):
    count, depth = rows.shape
    args = (rows, gate_vector, gate, up, dense_gate, *rest)
    return pl.pallas_call(
        units_kernel,
        out_shape=[
            pltpu.VMEM((count, gate.shape[1]), BF16),
            pltpu.VMEM((count, dense_gate.shape[0]), BF16),
        ],
        in_specs=[VMEM] * len(args),
        out_specs=[VMEM] * 2,
        compiler_params=params(8),
        cost_estimate=estimate(count, depth, 512),
        name="near_units",
    )(*map(in_vmem, args))


def far_terms(after, rows, *weights):
    return pl.pallas_call(
        branch_kernel,
        out_shape=pltpu.VMEM(rows.shape, BF16),
        in_specs=[ANY] + [VMEM] * (1 + len(weights)),
        out_specs=VMEM,
        compiler_params=params(8),
        cost_estimate=estimate(*rows.shape, 1024),
        name="far_terms",
    )(*map(in_vmem, (after, rows, *weights)))


def near_terms(units, dense, down, dense_down):
    args = (units, dense, down, dense_down)
    return pl.pallas_call(
        down_kernel,
        out_shape=pltpu.VMEM((units.shape[0], down.shape[1]), F32),
        in_specs=[VMEM] * 4,
        out_specs=VMEM,
        compiler_params=params(8),
        cost_estimate=estimate(units.shape[0], 512, down.shape[1]),
        name="near_terms",
    )(*map(in_vmem, args))


def last_kernel(parts, hidden, gain, shift, out):
    branches = parts[0].astype(F32)
    for i in range(1, parts.shape[0]):
        branches = branches + parts[i].astype(F32)
    rows = alpha_scale * hidden[0].astype(F32) + branches
    rows = normed(rows, rows.shape[1])
    width = out.shape[1]
    place = lax.axis_index("tp")
    own = rows[:, :width]
    for i in range(1, rows.shape[1] // width):
        own = jnp.where(place == i, rows[:, i * width : (i + 1) * width], own)
    out[...] = (own * gain[...] + shift[...]).astype(BF16)


def last_norm(parts, hidden, gain, shift):
    return pl.pallas_call(
        last_kernel,
        out_shape=jax.ShapeDtypeStruct((hidden.shape[1], gain.shape[1]), BF16),
        grid=(1,),
        in_specs=[
            VMEM,
            pl.BlockSpec((1, *hidden.shape[1:]), lambda i: (0, 0, 0)),
            VMEM,
            VMEM,
        ],
        out_specs=pl.BlockSpec((hidden.shape[1], gain.shape[1]), lambda i: (0, 0)),
        compiler_params=params(4),
        name="last_norm",
    )(parts, hidden, gain, shift)


def to_all(copies, axis):
    return lax.all_to_all(copies, axis, split_axis=0, concat_axis=0, tiled=True)


def per_device(
    tokens,
    w_query,
    w_key,
    w_value,
    w_forget,
    w_output,
    cache_keys,
    cache_values,
    cache_gates,
    lengths,
    ln1_gain,
    ln1_shift,
    gate_vector,
    dense_gate,
    dense_up,
    dense_down,
    expert_gate,
    expert_up,
    expert_down,
    expert_ids,
    expert_weights,
    ln2_gain,
    ln2_shift,
):
    kept = (
        expert_gate[0],
        expert_up[0],
        dense_gate.T,
        dense_up.T,
        expert_ids.T,
        expert_weights.T,
        expert_down[0],
        dense_down,
        ln1_gain[None],
        ln1_shift[None],
        ln2_gain[None],
        ln2_shift[None],
    )
    operands = (
        lengths,
        tokens,
        w_forget,
        cache_gates,
        w_query,
        w_key,
        w_value,
        w_output,
        cache_keys,
        cache_values,
    )
    heads, tokens, *kept = attend(lax.axis_size("tp"), operands, kept)
    unit_weights, down_weights = (gate_vector[None], *kept[:6]), kept[6:8]
    gain_1, shift_1, gain_2, shift_2 = kept[8:]
    plane = lax.axis_size(PLANE)
    copies = hidden_copies(plane, to_all(heads, "tp"), tokens, gain_1, shift_1)
    rows = to_all(copies, PLANE).reshape(-1, tokens.shape[1])
    rows_far = lax.ppermute(rows, "ep_2", OTHER_CORE)
    units, dense = near_units(rows, *unit_weights)
    terms_far = far_terms(units, rows_far, *unit_weights, *down_weights)
    terms_here = lax.ppermute(terms_far, "ep_2", OTHER_CORE)
    terms = near_terms(units, dense, *down_weights) + terms_here.astype(F32)
    arrived = to_all(terms.astype(BF16).reshape(plane, -1, terms.shape[1]), PLANE)
    owned = lax.optimization_barrier(arrived.astype(F32).sum(axis=0)).astype(BF16)
    parts = to_all(jnp.broadcast_to(owned, (lax.axis_size("tp"), *owned.shape)), "tp")
    return last_norm(parts, copies, gain_2, shift_2)


def solution(mesh):
    torus = Mesh(mesh.devices.reshape(8, 8, 2, mesh.shape["tp"]), ("ep_0", "ep_1", "ep_2", "tp"))
    in_specs = (
        P(EP, None),
        P(None, "tp"),
        P(None, "tp"),
        P(None, "tp"),
        P("tp", None),
        P("tp", None),
        P(EP, "tp", None, None),
        P(EP, "tp", None, None),
        P(EP, "tp", None),
        P(EP),
        P(),
        P(),
        P(),
        P(None, EP_TP),
        P(None, EP_TP),
        P(EP_TP, None),
        P(EP, None, "tp"),
        P(EP, None, "tp"),
        P(EP, "tp", None),
        P(),
        P(),
        P("tp"),
        P("tp"),
    )
    out_specs = P(EP, "tp")
    return jax.shard_map(
        per_device, mesh=torus, in_specs=in_specs, out_specs=out_specs, check_vma=False
    )
```

```python
import functools

import jax
import jax.numpy as jnp
from jax import lax
from jax.experimental import pallas as pl
from jax.experimental.pallas import tpu as pltpu
from jax.sharding import Mesh
from jax.sharding import PartitionSpec as P

EP = ("ep_0", "ep_1", "ep_2")
EP_TP = ("ep_0", "ep_1", "ep_2", "tp")
PLANE = ("ep_0", "ep_1")
OTHER_CORE = ((0, 1), (1, 0))

alpha_scale = 1.4142135623730951
norm_eps = 1e-05

F32 = jnp.float32
BF16 = jnp.bfloat16
ANY = pl.BlockSpec(memory_space=pl.ANY)
VMEM = pl.BlockSpec(memory_space=pltpu.VMEM)
SMEM = pl.BlockSpec(memory_space=pltpu.SMEM)
NT = (((1,), (1,)), ((), ()))


def dot(a, b):
    return jnp.dot(a, b, preferred_element_type=F32)


def dot_nt(a, b):
    return lax.dot_general(a, b, NT, preferred_element_type=F32)


def in_vmem(x):
    return pltpu.with_memory_space_constraint(x, pltpu.VMEM)


def params(mib):
    return pltpu.CompilerParams(vmem_limit_bytes=mib << 20)


def attend_kernel(
    lengths_hbm,
    tokens_hbm,
    w_forget_hbm,
    cache_gates_hbm,
    w_query,
    w_key,
    w_value,
    w_output,
    cache_keys,
    cache_values,
    *rest,
):
    kept = (len(rest) - 12) // 2
    sources, (terms, tokens, *places) = rest[:kept], rest[kept : 2 * kept + 1]
    scratch = rest[2 * kept + 1 :]
    lengths, w_forget, cache_gates, q_v, k_v, v_v, o_v, keys_v, values_v, sems, kept_sems = scratch
    width = w_query.shape[1]
    moves = [
        pltpu.make_async_copy(src, dst, sems.at[i])
        for i, (src, dst) in enumerate(
            (
                (tokens_hbm, tokens),
                (w_forget_hbm, w_forget),
                (lengths_hbm, lengths),
                (cache_gates_hbm, cache_gates),
                (w_query, q_v),
                (cache_keys, keys_v),
                (w_key, k_v),
                (cache_values, values_v),
                (w_value, v_v),
                (w_output, o_v),
            )
        )
    ]
    targets = list(places)
    dense_front = places[0]
    rows = dense_front.shape[0] // 2
    targets[:1] = (dense_front.at[:rows], dense_front.at[rows:])
    kept_moves = [
        pltpu.make_async_copy(src, dst, kept_sems.at[i])
        for i, (src, dst) in enumerate(zip(sources, targets))
    ]
    for move in moves + kept_moves:
        move.start()

    for move in moves[:4]:
        move.wait()
    x = tokens[...]
    scale = width ** (-0.5)
    length = cache_gates.shape[2]
    forget = jnp.sum(x.astype(F32) * w_forget[...].astype(F32), axis=1, keepdims=True)
    forget_new = jax.nn.log_sigmoid(forget)
    second = lax.broadcasted_iota(jnp.int32, (2, 1), 0) == 1
    used = jnp.where(second, lengths[1], lengths[0])
    gates = jnp.where(second, cache_gates[1], cache_gates[0])
    positions = lax.broadcasted_iota(jnp.int32, (2, length), 1)
    last_gate = jnp.sum(jnp.where(positions == used - 1, gates, 0.0), axis=1, keepdims=True)
    decay_bias = (last_gate + forget_new) - gates

    moves[4].wait()
    query = dot(x, q_v[...]).astype(BF16)
    moves[5].wait()
    scores = jnp.where(second, dot_nt(query, keys_v[1, 0]), dot_nt(query, keys_v[0, 0])) * scale
    scores = jnp.where(positions < used, scores + decay_bias, -jnp.inf)
    moves[6].wait()
    new_key = dot(x, k_v[...]).astype(BF16)
    own_score = (
        jnp.sum(query.astype(F32) * new_key.astype(F32), axis=1, keepdims=True) * scale
    )
    peak = jnp.maximum(jnp.max(scores, axis=1, keepdims=True), own_score)
    exp_terms = jnp.exp(scores - peak)
    own_exp = jnp.exp(own_score - peak)
    denominator = jnp.sum(exp_terms, axis=1, keepdims=True) + own_exp
    probs = (exp_terms / denominator).astype(BF16)
    own_prob = (own_exp / denominator).astype(BF16)
    moves[7].wait()
    weighted = jnp.where(second, dot(probs, values_v[1, 0]), dot(probs, values_v[0, 0]))
    moves[8].wait()
    new_value = dot(x, v_v[...]).astype(BF16)
    weighted = weighted + own_prob.astype(F32) * new_value.astype(F32)
    moves[9].wait()
    term = dot(weighted.astype(BF16), o_v[...]).astype(BF16)
    for i in range(terms.shape[0]):
        terms[i] = term
    for move in kept_moves:
        move.wait()


def attend(copies, operands, kept):
    operands = [pltpu.with_memory_space_constraint(a, pltpu.HBM) for a in (*operands, *kept)]
    lengths, tokens, w_forget, gates, w_query, w_key, w_value, w_output, keys, values = operands[:10]
    dense_gate, dense_up = kept[:2]
    joined = ((2 * dense_gate.shape[0], dense_gate.shape[1]),)
    held = (w_forget, gates, w_query, w_key, w_value, w_output, keys, values)
    return pl.pallas_call(
        attend_kernel,
        out_shape=[pltpu.VMEM((copies, tokens.shape[0], w_output.shape[1]), BF16)]
        + [pltpu.VMEM(tokens.shape, BF16)]
        + [pltpu.VMEM(shape, BF16) for shape in joined]
        + [pltpu.VMEM(a.shape, a.dtype) for a in kept[2:]],
        in_specs=[pl.BlockSpec(memory_space=pltpu.HBM)] * len(operands),
        out_specs=[VMEM] * (len(kept) + 1),
        scratch_shapes=[
            pltpu.SMEM(lengths.shape, jnp.int32),
            *(pltpu.VMEM(a.shape, a.dtype) for a in held),
            pltpu.SemaphoreType.DMA((10,)),
            pltpu.SemaphoreType.DMA((len(kept),)),
        ],
        compiler_params=params(12),
        name="attend",
    )(*operands)


def normed(rows, width):
    row_mean = jnp.sum(rows, axis=-1, keepdims=True) * (1.0 / width)
    row_var = jnp.sum(rows * rows, axis=-1, keepdims=True) * (1.0 / width) - row_mean * row_mean
    return (rows - row_mean) * lax.rsqrt(row_var + norm_eps)


def hidden_kernel(heads, tokens, gain, shift, copies):
    attention = heads[0].astype(F32)
    for i in range(1, heads.shape[0]):
        attention = attention + heads[i].astype(F32)
    rows = alpha_scale * tokens[...].astype(F32) + attention
    hidden = (normed(rows, rows.shape[1]) * gain[...] + shift[...]).astype(BF16)
    for i in range(copies.shape[0]):
        copies[i] = hidden


def hidden_copies(count, heads, tokens, gain, shift):
    return pl.pallas_call(
        hidden_kernel,
        out_shape=pltpu.VMEM((count, *tokens.shape), BF16),
        in_specs=[VMEM] * 4,
        out_specs=VMEM,
        compiler_params=params(4),
        name="hidden_copies",
    )(in_vmem(heads), tokens, in_vmem(gain), in_vmem(shift))


def unit_values(far, rows, gate_vector, front, dense_front, ids, shares):
    tokens = ids.shape[1]
    core = lax.axis_index("ep_2")
    expert = (lax.axis_index("ep_0") * lax.axis_size("ep_1") + lax.axis_index("ep_1")) * 2 + core
    side = 1 - core if far else core
    x = rows[...].reshape(-1, rows.shape[2])
    count = x.shape[0]
    both = [dot(x, w[...]) for w in front]
    dense_both = dot_nt(x, dense_front[...])
    picked = jnp.where(ids[...] == expert, shares[...], 0.0)
    share_row = picked[0:1] + picked[1:2]
    row = lax.broadcasted_iota(jnp.int32, (count, tokens), 0)
    column = lax.broadcasted_iota(jnp.int32, (count, tokens), 1)
    match = column == 4 * (row >> 1) + 2 * side + (row & 1)
    share = jnp.sum(jnp.where(match, share_row, 0.0), axis=1, keepdims=True)
    mixed = jnp.sum(x.astype(F32) * gate_vector[...].astype(F32), axis=1, keepdims=True)
    mixing = 1.0 / (1.0 + jnp.exp(-mixed))
    a, b = halves(both[0]) if len(both) == 1 else both
    units = (a / (1.0 + jnp.exp(-a)) * b * share).astype(BF16)
    a, b = halves(dense_both)
    dense = (a / (1.0 + jnp.exp(-a)) * b * mixing).astype(BF16)
    return jnp.concatenate([units, dense], axis=1)


def halves(x):
    half = x.shape[1] // 2
    return x[:, :half], x[:, half:]


def units_kernel(
    rows,
    gate_vector,
    gate,
    up,
    expert_down,
    dense_down,
    dense_front,
    ids,
    shares,
    units,
    front,
    down,
):
    units[...] = unit_values(False, rows, gate_vector, (gate, up), dense_front, ids, shares)
    width, depth = gate.shape[1], expert_down.shape[0]
    front[:, :width] = gate[...]
    front[:, width:] = up[...]
    down[:depth] = expert_down[...]
    down[depth:] = dense_down[...]


def branch_kernel(rows, gate_vector, front, down, dense_front, ids, shares, terms):
    units = unit_values(True, rows, gate_vector, (front,), dense_front, ids, shares)
    terms[...] = dot(units, down[...]).astype(BF16)


def down_kernel(units, down, terms):
    terms[...] = dot(units[...], down[...])


def add_kernel(near, far, terms):
    terms[...] = (near[...] + far[...].astype(F32)).astype(BF16).reshape(terms.shape)


def collect_kernel(terms, copies):
    kept, width = terms.shape[1:]
    rows = terms[...].reshape(-1, width)
    column = lax.broadcasted_iota(jnp.int32, (kept, rows.shape[0]), 1)
    row = lax.broadcasted_iota(jnp.int32, (kept, rows.shape[0]), 0)
    total = dot(jnp.where(lax.rem(column, kept) == row, 1.0, 0.0).astype(BF16), rows)
    total = total.astype(BF16)
    for i in range(copies.shape[0]):
        copies[i] = total


def estimate(rows, depth, columns):
    return pl.CostEstimate(
        flops=2 * rows * depth * columns, bytes_accessed=4096, transcendentals=0
    )


def near_units(rows, gate_vector, gate, up, expert_down, dense_down, *rest):
    args = (rows, gate_vector, gate, up, expert_down, dense_down, *rest)
    count, depth = rows.size // rows.shape[-1], expert_down.shape[0] + dense_down.shape[0]
    return pl.pallas_call(
        units_kernel,
        out_shape=[
            pltpu.VMEM((count, depth), BF16),
            pltpu.VMEM((gate.shape[0], 2 * gate.shape[1]), BF16),
            pltpu.VMEM((depth, expert_down.shape[1]), BF16),
        ],
        in_specs=[VMEM] * len(args),
        out_specs=[VMEM] * 3,
        compiler_params=params(8),
        cost_estimate=estimate(count, rows.shape[-1], 512),
        name="near_units",
    )(*map(in_vmem, args))


def far_terms(rows, *weights):
    count = rows.size // rows.shape[-1]
    return pl.pallas_call(
        branch_kernel,
        out_shape=pltpu.VMEM((count, rows.shape[-1]), BF16),
        in_specs=[VMEM] * (1 + len(weights)),
        out_specs=VMEM,
        compiler_params=params(8),
        cost_estimate=estimate(count, rows.shape[-1], 1024),
        name="far_terms",
    )(*map(in_vmem, (rows, *weights)))


def near_terms(units, down):
    return pl.pallas_call(
        down_kernel,
        out_shape=pltpu.VMEM((units.shape[0], down.shape[1]), F32),
        in_specs=[VMEM] * 2,
        out_specs=VMEM,
        compiler_params=params(8),
        cost_estimate=estimate(units.shape[0], 512, down.shape[1]),
        name="near_terms",
    )(*map(in_vmem, (units, down)))


def added(shape, near, far):
    return pl.pallas_call(
        add_kernel,
        out_shape=pltpu.VMEM(shape, BF16),
        in_specs=[VMEM] * 2,
        out_specs=VMEM,
        compiler_params=params(8),
        name="added",
    )(*map(in_vmem, (near, far)))


def collected(count, terms):
    return pl.pallas_call(
        collect_kernel,
        out_shape=pltpu.VMEM((count, *terms.shape[1:]), BF16),
        in_specs=[VMEM],
        out_specs=VMEM,
        compiler_params=params(8),
        name="collected",
    )(in_vmem(terms))


def last_kernel(parts, hidden, gain, shift, out):
    branches = parts[0].astype(F32)
    for i in range(1, parts.shape[0]):
        branches = branches + parts[i].astype(F32)
    rows = alpha_scale * hidden[0].astype(F32) + branches
    rows = normed(rows, rows.shape[1])
    width = out.shape[1]
    place = lax.axis_index("tp")
    own = rows[:, :width]
    for i in range(1, rows.shape[1] // width):
        own = jnp.where(place == i, rows[:, i * width : (i + 1) * width], own)
    out[...] = (own * gain[...] + shift[...]).astype(BF16)


def last_norm(parts, hidden, gain, shift):
    return pl.pallas_call(
        last_kernel,
        out_shape=jax.ShapeDtypeStruct((hidden.shape[1], gain.shape[1]), BF16),
        in_specs=[VMEM] * 4,
        out_specs=VMEM,
        compiler_params=params(4),
        name="last_norm",
    )(*map(in_vmem, (parts, hidden, gain, shift)))


def to_all(copies, axis):
    return lax.all_to_all(copies, axis, split_axis=0, concat_axis=0, tiled=True)


def per_device(
    tokens,
    w_query,
    w_key,
    w_value,
    w_forget,
    w_output,
    cache_keys,
    cache_values,
    cache_gates,
    lengths,
    ln1_gain,
    ln1_shift,
    gate_vector,
    dense_gate,
    dense_up,
    dense_down,
    expert_gate,
    expert_up,
    expert_down,
    expert_ids,
    expert_weights,
    ln2_gain,
    ln2_shift,
):
    kept = (
        dense_gate.T,
        dense_up.T,
        expert_ids.T,
        expert_weights.T,
        ln1_gain[None],
        ln1_shift[None],
        ln2_gain[None],
        ln2_shift[None],
    )
    operands = (
        lengths,
        tokens,
        w_forget,
        cache_gates,
        w_query,
        w_key,
        w_value,
        w_output,
        cache_keys,
        cache_values,
    )
    heads, tokens, *kept = attend(lax.axis_size("tp"), operands, kept)
    dense_front, ids, shares, gain_1, shift_1, gain_2, shift_2 = kept
    plane = lax.axis_size(PLANE)
    copies = hidden_copies(plane, to_all(heads, "tp"), tokens, gain_1, shift_1)
    rows = to_all(copies, PLANE)
    rows_far = lax.ppermute(rows, "ep_2", OTHER_CORE)
    tail = (dense_front, ids, shares)
    vector = gate_vector[None]
    units, front, down = near_units(
        rows, vector, expert_gate[0], expert_up[0], expert_down[0], dense_down, *tail
    )
    terms_far = far_terms(rows_far, vector, front, down, *tail)
    terms_here = lax.ppermute(terms_far, "ep_2", OTHER_CORE)
    terms = added(copies.shape, near_terms(units, down), terms_here)
    parts = to_all(collected(lax.axis_size("tp"), to_all(terms, PLANE)), "tp")
    return last_norm(parts, copies, gain_2, shift_2)


def solution(mesh):
    torus = Mesh(mesh.devices.reshape(8, 8, 2, mesh.shape["tp"]), ("ep_0", "ep_1", "ep_2", "tp"))
    in_specs = (
        P(EP, None),
        P(None, "tp"),
        P(None, "tp"),
        P(None, "tp"),
        P("tp", None),
        P("tp", None),
        P(EP, "tp", None, None),
        P(EP, "tp", None, None),
        P(EP, "tp", None),
        P(EP),
        P(),
        P(),
        P(),
        P(None, EP_TP),
        P(None, EP_TP),
        P(EP_TP, None),
        P(EP, None, "tp"),
        P(EP, None, "tp"),
        P(EP, "tp", None),
        P(),
        P(),
        P("tp"),
        P("tp"),
    )
    out_specs = P(EP, "tp")
    return jax.shard_map(
        per_device, mesh=torus, in_specs=in_specs, out_specs=out_specs, check_vma=False
    )
```

```python
import functools

import jax
import jax.numpy as jnp
from jax import lax
from jax.experimental import pallas as pl
from jax.experimental.pallas import tpu as pltpu
from jax.sharding import Mesh
from jax.sharding import PartitionSpec as P

EP = ("ep_0", "ep_1", "ep_2")
EP_TP = ("ep_0", "ep_1", "ep_2", "tp")
OTHER_CORE = ((0, 1), (1, 0))

alpha_scale = 1.4142135623730951
norm_eps = 1e-05

F32 = jnp.float32
BF16 = jnp.bfloat16
ANY = pl.BlockSpec(memory_space=pl.ANY)
VMEM = pl.BlockSpec(memory_space=pltpu.VMEM)
SMEM = pl.BlockSpec(memory_space=pltpu.SMEM)
NT = (((1,), (1,)), ((), ()))


def dot(a, b):
    return jnp.dot(a, b, preferred_element_type=F32)


def dot_nt(a, b):
    return lax.dot_general(a, b, NT, preferred_element_type=F32)


def in_vmem(x):
    return pltpu.with_memory_space_constraint(x, pltpu.VMEM)


def params(mib):
    return pltpu.CompilerParams(vmem_limit_bytes=mib << 20)


def attend_kernel(
    lengths_hbm,
    tokens_hbm,
    w_forget_hbm,
    cache_gates_hbm,
    w_query,
    w_key,
    w_value,
    w_output,
    cache_keys,
    cache_values,
    *rest,
):
    kept = (len(rest) - 12) // 2
    sources, (terms, *places) = rest[:kept], rest[kept : 2 * kept]
    scratch = rest[2 * kept :]
    lengths, tokens, w_forget, cache_gates, q_v, k_v, v_v, o_v, keys_v, values_v, sems, kept_sems = scratch
    width = w_query.shape[1]
    moves = [
        pltpu.make_async_copy(src, dst, sems.at[i])
        for i, (src, dst) in enumerate(
            (
                (tokens_hbm, tokens),
                (w_forget_hbm, w_forget),
                (lengths_hbm, lengths),
                (cache_gates_hbm, cache_gates),
                (w_query, q_v),
                (cache_keys, keys_v),
                (w_key, k_v),
                (cache_values, values_v),
                (w_value, v_v),
                (w_output, o_v),
            )
        )
    ]
    targets = list(places)
    dense_front = places[0]
    rows = dense_front.shape[0] // 2
    targets[:1] = (dense_front.at[:rows], dense_front.at[rows:])
    kept_moves = [
        pltpu.make_async_copy(src, dst, kept_sems.at[i])
        for i, (src, dst) in enumerate(zip(sources, targets))
    ]
    for move in moves + kept_moves:
        move.start()

    for move in moves[:4]:
        move.wait()
    x = tokens[...]
    scale = width ** (-0.5)
    length = cache_gates.shape[2]
    forget = jnp.sum(x.astype(F32) * w_forget[...].astype(F32), axis=1, keepdims=True)
    forget_new = jax.nn.log_sigmoid(forget)
    second = lax.broadcasted_iota(jnp.int32, (2, 1), 0) == 1
    used = jnp.where(second, lengths[1], lengths[0])
    gates = jnp.where(second, cache_gates[1], cache_gates[0])
    positions = lax.broadcasted_iota(jnp.int32, (2, length), 1)
    last_gate = jnp.sum(jnp.where(positions == used - 1, gates, 0.0), axis=1, keepdims=True)
    decay_bias = (last_gate + forget_new) - gates

    moves[4].wait()
    query = dot(x, q_v[...]).astype(BF16)
    moves[5].wait()
    scores = jnp.where(second, dot_nt(query, keys_v[1, 0]), dot_nt(query, keys_v[0, 0])) * scale
    scores = jnp.where(positions < used, scores + decay_bias, -jnp.inf)
    moves[6].wait()
    new_key = dot(x, k_v[...]).astype(BF16)
    own_score = (
        jnp.sum(query.astype(F32) * new_key.astype(F32), axis=1, keepdims=True) * scale
    )
    peak = jnp.maximum(jnp.max(scores, axis=1, keepdims=True), own_score)
    exp_terms = jnp.exp(scores - peak)
    own_exp = jnp.exp(own_score - peak)
    denominator = jnp.sum(exp_terms, axis=1, keepdims=True) + own_exp
    probs = (exp_terms / denominator).astype(BF16)
    own_prob = (own_exp / denominator).astype(BF16)
    moves[7].wait()
    weighted = jnp.where(second, dot(probs, values_v[1, 0]), dot(probs, values_v[0, 0]))
    moves[8].wait()
    new_value = dot(x, v_v[...]).astype(BF16)
    weighted = weighted + own_prob.astype(F32) * new_value.astype(F32)
    moves[9].wait()
    term = dot(weighted.astype(BF16), o_v[...])
    term = (term + (alpha_scale / lax.axis_size("tp")) * x.astype(F32)).astype(BF16)
    for i in range(terms.shape[0]):
        terms[i] = term
    for move in kept_moves:
        move.wait()


def attend(copies, operands, kept):
    operands = [pltpu.with_memory_space_constraint(a, pltpu.HBM) for a in (*operands, *kept)]
    lengths, tokens, w_forget, gates, w_query, w_key, w_value, w_output, keys, values = operands[:10]
    dense_gate, dense_up = kept[:2]
    joined = ((2 * dense_gate.shape[0], dense_gate.shape[1]),)
    held = (tokens, w_forget, gates, w_query, w_key, w_value, w_output, keys, values)
    return pl.pallas_call(
        attend_kernel,
        out_shape=[pltpu.VMEM((copies, tokens.shape[0], w_output.shape[1]), BF16)]
        + [pltpu.VMEM(shape, BF16) for shape in joined]
        + [pltpu.VMEM(a.shape, a.dtype) for a in kept[2:]],
        in_specs=[pl.BlockSpec(memory_space=pltpu.HBM)] * len(operands),
        out_specs=[VMEM] * len(kept),
        scratch_shapes=[
            pltpu.SMEM(lengths.shape, jnp.int32),
            *(pltpu.VMEM(a.shape, a.dtype) for a in held),
            pltpu.SemaphoreType.DMA((10,)),
            pltpu.SemaphoreType.DMA((len(kept),)),
        ],
        compiler_params=params(12),
        name="attend",
    )(*operands)


def normed(rows, width):
    row_mean = jnp.sum(rows, axis=-1, keepdims=True) * (1.0 / width)
    row_var = jnp.sum(rows * rows, axis=-1, keepdims=True) * (1.0 / width) - row_mean * row_mean
    return (rows - row_mean) * lax.rsqrt(row_var + norm_eps)


def picking(shape, rule):
    row = lax.broadcasted_iota(jnp.int32, shape, 0)
    column = lax.broadcasted_iota(jnp.int32, shape, 1)
    return jnp.where(rule(row, column), 1.0, 0.0).astype(BF16)


def hidden_kernel(heads, gain, shift, copies):
    kept, width = heads.shape[1:]
    terms = heads[...].reshape(-1, width)
    rows = copies.shape[1]
    spread = terms.shape[0] // rows
    pick = picking(
        (rows, terms.shape[0]),
        lambda i, j: (i // kept == j // (kept * spread)) & (lax.rem(i, kept) == lax.rem(j, kept)),
    )
    rows = dot(pick, terms)
    hidden = (normed(rows, width) * gain[...] + shift[...]).astype(BF16)
    for i in range(copies.shape[0]):
        copies[i] = hidden


def hidden_copies(side, heads, gain, shift):
    kept, width = heads.shape[1:]
    return pl.pallas_call(
        hidden_kernel,
        out_shape=pltpu.VMEM((side, side * kept, width), BF16),
        in_specs=[VMEM] * 3,
        out_specs=VMEM,
        compiler_params=params(4),
        name="hidden_copies",
    )(*map(in_vmem, (heads, gain, shift)))


def unit_values(far, rows, gate_vector, front, dense_front, ids, shares):
    tokens = ids.shape[1]
    core = lax.axis_index("ep_2")
    expert = (lax.axis_index("ep_0") * lax.axis_size("ep_1") + lax.axis_index("ep_1")) * 2 + core
    side = 1 - core if far else core
    x = rows[...]
    count = x.shape[0]
    both = [dot(x, w[...]) for w in front]
    dense_both = dot_nt(x, dense_front[...])
    picked = jnp.where(ids[...] == expert, shares[...], 0.0)
    share_row = picked[0:1] + picked[1:2]
    row = lax.broadcasted_iota(jnp.int32, (count, tokens), 0)
    column = lax.broadcasted_iota(jnp.int32, (count, tokens), 1)
    line = lax.axis_size("ep_0")
    outer, inner = row // (2 * line), (row // 2) % line
    far_z = jnp.where(side == 0, inner, outer)
    far_y = jnp.where(side == 0, outer, inner)
    match = column == 4 * (far_z * line + far_y) + 2 * side + (row & 1)
    share = jnp.sum(jnp.where(match, share_row, 0.0), axis=1, keepdims=True)
    mixed = jnp.sum(x.astype(F32) * gate_vector[...].astype(F32), axis=1, keepdims=True)
    mixing = 1.0 / (1.0 + jnp.exp(-mixed))
    a, b = halves(both[0]) if len(both) == 1 else both
    units = (a / (1.0 + jnp.exp(-a)) * b * share).astype(BF16)
    a, b = halves(dense_both)
    dense = (a / (1.0 + jnp.exp(-a)) * b * mixing).astype(BF16)
    return jnp.concatenate([units, dense], axis=1)


def halves(x):
    half = x.shape[1] // 2
    return x[:, :half], x[:, half:]


def units_kernel(
    rows,
    gate_vector,
    gate,
    up,
    expert_down,
    dense_down,
    dense_front,
    ids,
    shares,
    units,
    front,
    down,
):
    units[...] = unit_values(False, rows, gate_vector, (gate, up), dense_front, ids, shares)
    width, depth = gate.shape[1], expert_down.shape[0]
    front[:, :width] = gate[...]
    front[:, width:] = up[...]
    down[:depth] = expert_down[...]
    down[depth:] = dense_down[...]


def branch_kernel(rows, gate_vector, front, down, dense_front, ids, shares, terms):
    units = unit_values(True, rows, gate_vector, (front,), dense_front, ids, shares)
    terms[...] = dot(units, down[...]).astype(BF16)


def down_kernel(units, down, terms):
    terms[...] = dot(units[...], down[...])


def add_kernel(near, far, terms):
    terms[...] = (near[...] + far[...].astype(F32)).astype(BF16)


def collect_kernel(terms, copies):
    total = terms[0].astype(F32)
    for i in range(1, terms.shape[0]):
        total = total + terms[i].astype(F32)
    total = total.astype(BF16).reshape(copies.shape[0], *copies.shape[2:])
    for i in range(copies.shape[1]):
        copies[:, i] = total


def estimate(rows, depth, columns):
    return pl.CostEstimate(
        flops=2 * rows * depth * columns, bytes_accessed=4096, transcendentals=0
    )


def near_units(rows, gate_vector, gate, up, expert_down, dense_down, *rest):
    args = (rows, gate_vector, gate, up, expert_down, dense_down, *rest)
    count, depth = rows.size // rows.shape[-1], expert_down.shape[0] + dense_down.shape[0]
    return pl.pallas_call(
        units_kernel,
        out_shape=[
            pltpu.VMEM((count, depth), BF16),
            pltpu.VMEM((gate.shape[0], 2 * gate.shape[1]), BF16),
            pltpu.VMEM((depth, expert_down.shape[1]), BF16),
        ],
        in_specs=[VMEM] * len(args),
        out_specs=[VMEM] * 3,
        compiler_params=params(8),
        cost_estimate=estimate(count, rows.shape[-1], 512),
        name="near_units",
    )(*map(in_vmem, args))


def far_terms(rows, *weights):
    count = rows.size // rows.shape[-1]
    return pl.pallas_call(
        branch_kernel,
        out_shape=pltpu.VMEM((count, rows.shape[-1]), BF16),
        in_specs=[VMEM] * (1 + len(weights)),
        out_specs=VMEM,
        compiler_params=params(8),
        cost_estimate=estimate(count, rows.shape[-1], 1024),
        name="far_terms",
    )(*map(in_vmem, (rows, *weights)))


def near_terms(units, down):
    return pl.pallas_call(
        down_kernel,
        out_shape=pltpu.VMEM((units.shape[0], down.shape[1]), F32),
        in_specs=[VMEM] * 2,
        out_specs=VMEM,
        compiler_params=params(8),
        cost_estimate=estimate(units.shape[0], 512, down.shape[1]),
        name="near_terms",
    )(*map(in_vmem, (units, down)))


def added(near, far):
    return pl.pallas_call(
        add_kernel,
        out_shape=pltpu.VMEM(far.shape, BF16),
        in_specs=[VMEM] * 2,
        out_specs=VMEM,
        compiler_params=params(8),
        name="added",
    )(*map(in_vmem, (near, far)))


def collected(count, terms):
    side, rows, width = terms.shape
    return pl.pallas_call(
        collect_kernel,
        out_shape=pltpu.VMEM((side, count, rows // side, width), BF16),
        in_specs=[VMEM],
        out_specs=VMEM,
        compiler_params=params(8),
        name="collected",
    )(in_vmem(terms))


def last_kernel(parts, hidden, gain, shift, out):
    kept = parts.shape[1]
    terms = parts[...].reshape(-1, parts.shape[2])
    core = lax.axis_index("ep_2")
    at = jnp.where(core == 0, lax.axis_index("ep_0"), lax.axis_index("ep_1"))
    pick = picking((kept, terms.shape[0]), lambda i, j: lax.rem(j, kept) == i)
    own = picking((kept, hidden.shape[1]), lambda i, j: j == at * kept + i)
    rows = alpha_scale * dot(own, hidden[0]) + dot(pick, terms)
    rows = normed(rows, rows.shape[1])
    width = out.shape[1]
    place = lax.axis_index("tp")
    own = rows[:, :width]
    for i in range(1, rows.shape[1] // width):
        own = jnp.where(place == i, rows[:, i * width : (i + 1) * width], own)
    out[...] = (own * gain[...] + shift[...]).astype(BF16)


def last_norm(parts, hidden, gain, shift):
    return pl.pallas_call(
        last_kernel,
        out_shape=jax.ShapeDtypeStruct((parts.shape[1], gain.shape[1]), BF16),
        in_specs=[VMEM] * 4,
        out_specs=VMEM,
        compiler_params=params(4),
        name="last_norm",
    )(*map(in_vmem, (parts, hidden, gain, shift)))


def lines(side, wide):
    z, y, c = (side * 2, 2, 1)
    alike = range(side)
    along_y = [[z * i + y * j for j in alike] for i in alike]
    along_z = [[z * i + y * j for i in alike] for j in alike]
    if wide:
        ways = range(wide)
        groups = along_z + [[g + c for g in group] for group in along_y]
        return [[g * wide + x for g in group for x in ways] for group in groups]
    return along_y + [[g + c for g in group] for group in along_z]


def along(array, side):
    return lax.all_to_all(array, EP, 0, 0, axis_index_groups=lines(side, 0), tiled=True)


def across(array, side, ways):
    groups = lines(side, ways)
    return lax.all_to_all(array, EP_TP, 0, 0, axis_index_groups=groups, tiled=True)


def per_device(
    tokens,
    w_query,
    w_key,
    w_value,
    w_forget,
    w_output,
    cache_keys,
    cache_values,
    cache_gates,
    lengths,
    ln1_gain,
    ln1_shift,
    gate_vector,
    dense_gate,
    dense_up,
    dense_down,
    expert_gate,
    expert_up,
    expert_down,
    expert_ids,
    expert_weights,
    ln2_gain,
    ln2_shift,
):
    kept = (
        dense_gate.T,
        dense_up.T,
        expert_ids.T,
        expert_weights.T,
        ln1_gain[None],
        ln1_shift[None],
        ln2_gain[None],
        ln2_shift[None],
    )
    operands = (
        lengths,
        tokens,
        w_forget,
        cache_gates,
        w_query,
        w_key,
        w_value,
        w_output,
        cache_keys,
        cache_values,
    )
    side, ways = lax.axis_size("ep_0"), lax.axis_size("tp")
    heads, *kept = attend(side * ways, operands, kept)
    dense_front, ids, shares, gain_1, shift_1, gain_2, shift_2 = kept
    copies = hidden_copies(side, across(heads, side, ways), gain_1, shift_1)
    rows = along(copies, side).reshape(-1, tokens.shape[1])
    rows_far = lax.ppermute(rows, "ep_2", OTHER_CORE)
    tail = (dense_front, ids, shares)
    vector = gate_vector[None]
    units, front, down = near_units(
        rows, vector, expert_gate[0], expert_up[0], expert_down[0], dense_down, *tail
    )
    terms_far = far_terms(rows_far, vector, front, down, *tail)
    terms_here = lax.ppermute(terms_far, "ep_2", OTHER_CORE)
    terms = added(near_terms(units, down), terms_here).reshape(copies.shape)
    sums = collected(ways, along(terms, side))
    parts = across(sums.reshape(-1, *sums.shape[2:]), side, ways)
    return last_norm(parts, copies, gain_2, shift_2)


def solution(mesh):
    torus = Mesh(mesh.devices.reshape(8, 8, 2, mesh.shape["tp"]), ("ep_0", "ep_1", "ep_2", "tp"))
    in_specs = (
        P(EP, None),
        P(None, "tp"),
        P(None, "tp"),
        P(None, "tp"),
        P("tp", None),
        P("tp", None),
        P(EP, "tp", None, None),
        P(EP, "tp", None, None),
        P(EP, "tp", None),
        P(EP),
        P(),
        P(),
        P(),
        P(None, EP_TP),
        P(None, EP_TP),
        P(EP_TP, None),
        P(EP, None, "tp"),
        P(EP, None, "tp"),
        P(EP, "tp", None),
        P(),
        P(),
        P("tp"),
        P("tp"),
    )
    out_specs = P(EP, "tp")
    return jax.shard_map(
        per_device, mesh=torus, in_specs=in_specs, out_specs=out_specs, check_vma=False
    )
```

```python
import functools

import jax
import jax.numpy as jnp
from jax import lax
from jax.experimental import pallas as pl
from jax.experimental.pallas import tpu as pltpu
from jax.sharding import Mesh
from jax.sharding import PartitionSpec as P

EP = ("ep_0", "ep_1", "ep_2")
EP_TP = ("ep_0", "ep_1", "ep_2", "tp")
OTHER_CORE = ((0, 1), (1, 0))

EXPERT_UNITS = 128
DENSE_UNITS = 16
alpha_scale = 1.4142135623730951
norm_eps = 1e-05

F32 = jnp.float32
BF16 = jnp.bfloat16
ANY = pl.BlockSpec(memory_space=pl.ANY)
VMEM = pl.BlockSpec(memory_space=pltpu.VMEM)
SMEM = pl.BlockSpec(memory_space=pltpu.SMEM)
NT = (((1,), (1,)), ((), ()))


def dot(a, b):
    return jnp.dot(a, b, preferred_element_type=F32)


def dot_nt(a, b):
    return lax.dot_general(a, b, NT, preferred_element_type=F32)


def in_vmem(x):
    return pltpu.with_memory_space_constraint(x, pltpu.VMEM)


def params(mib):
    return pltpu.CompilerParams(vmem_limit_bytes=mib << 20)


def attend_kernel(
    lengths_hbm,
    tokens_hbm,
    w_forget_hbm,
    cache_gates_hbm,
    w_query,
    w_key,
    w_value,
    w_output,
    cache_keys,
    cache_values,
    *rest,
):
    kept = (len(rest) - 8) // 2
    sources, (terms, *places) = rest[:kept], rest[kept : 2 * kept - 4]
    scratch = rest[2 * kept - 4 :]
    lengths, tokens, w_forget, cache_gates, q_v, k_v, v_v, o_v, keys_v, values_v, sems, kept_sems = scratch
    width = w_query.shape[1]
    moves = [
        pltpu.make_async_copy(src, dst, sems.at[i])
        for i, (src, dst) in enumerate(
            (
                (tokens_hbm, tokens),
                (w_forget_hbm, w_forget),
                (lengths_hbm, lengths),
                (cache_gates_hbm, cache_gates),
                (w_query, q_v),
                (cache_keys, keys_v),
                (w_key, k_v),
                (cache_values, values_v),
                (w_value, v_v),
                (w_output, o_v),
            )
        )
    ]
    targets = list(places)
    pool = places[0]
    gate, up, down, *dense = sources[:6]
    depth, width_up = pool.shape[1], gate.shape[1]
    rows = gate.shape[0] * 2 * width_up // depth
    pieces = []
    for k in range(gate.shape[0] // rows):
        for n, source in enumerate((gate, up)):
            start = (2 * k + n) * width_up
            pieces.append(
                (source.at[rows * k : rows * (k + 1)], pool.at[:rows, start : start + width_up])
            )
    for source in (down, *dense):
        pieces.append((source, pool.at[rows : rows + source.shape[0]]))
        rows += source.shape[0]
    pieces += zip(sources[6:], places[1:])
    kept_moves = [
        pltpu.make_async_copy(src, dst, kept_sems.at[i])
        for i, (src, dst) in enumerate(pieces)
    ]
    for move in moves + kept_moves:
        move.start()

    for move in moves[:4]:
        move.wait()
    x = tokens[...]
    scale = width ** (-0.5)
    length = cache_gates.shape[2]
    forget = jnp.sum(x.astype(F32) * w_forget[...].astype(F32), axis=1, keepdims=True)
    forget_new = jax.nn.log_sigmoid(forget)
    second = lax.broadcasted_iota(jnp.int32, (2, 1), 0) == 1
    used = jnp.where(second, lengths[1], lengths[0])
    gates = jnp.where(second, cache_gates[1], cache_gates[0])
    positions = lax.broadcasted_iota(jnp.int32, (2, length), 1)
    last_gate = jnp.sum(jnp.where(positions == used - 1, gates, 0.0), axis=1, keepdims=True)
    decay_bias = (last_gate + forget_new) - gates

    moves[4].wait()
    query = dot(x, q_v[...]).astype(BF16)
    moves[5].wait()
    scores = jnp.where(second, dot_nt(query, keys_v[1, 0]), dot_nt(query, keys_v[0, 0])) * scale
    scores = jnp.where(positions < used, scores + decay_bias, -jnp.inf)
    moves[6].wait()
    new_key = dot(x, k_v[...]).astype(BF16)
    own_score = (
        jnp.sum(query.astype(F32) * new_key.astype(F32), axis=1, keepdims=True) * scale
    )
    peak = jnp.maximum(jnp.max(scores, axis=1, keepdims=True), own_score)
    exp_terms = jnp.exp(scores - peak)
    own_exp = jnp.exp(own_score - peak)
    denominator = jnp.sum(exp_terms, axis=1, keepdims=True) + own_exp
    probs = (exp_terms / denominator).astype(BF16)
    own_prob = (own_exp / denominator).astype(BF16)
    moves[7].wait()
    weighted = jnp.where(second, dot(probs, values_v[1, 0]), dot(probs, values_v[0, 0]))
    moves[8].wait()
    new_value = dot(x, v_v[...]).astype(BF16)
    weighted = weighted + own_prob.astype(F32) * new_value.astype(F32)
    moves[9].wait()
    term = dot(weighted.astype(BF16), o_v[...])
    term = (term + (alpha_scale / lax.axis_size("tp")) * x.astype(F32)).astype(BF16)
    for i in range(terms.shape[0]):
        terms[i] = term
    for move in kept_moves:
        move.wait()


def rows_of(gate, line):
    return 2 * gate.size // line


def attend(copies, operands, kept):
    operands = [pltpu.with_memory_space_constraint(a, pltpu.HBM) for a in (*operands, *kept)]
    lengths, tokens, w_forget, gates, w_query, w_key, w_value, w_output, keys, values = operands[:10]
    gate, up, down, *dense = kept[:6]
    line = down.shape[1]
    rows = (gate.size + up.size) // line + down.shape[0] + sum(a.shape[0] for a in dense)
    held = (tokens, w_forget, gates, w_query, w_key, w_value, w_output, keys, values)
    return pl.pallas_call(
        attend_kernel,
        out_shape=[pltpu.VMEM((copies, tokens.shape[0], w_output.shape[1]), BF16)]
        + [pltpu.VMEM((rows, line), BF16)]
        + [pltpu.VMEM(a.shape, a.dtype) for a in kept[6:]],
        in_specs=[pl.BlockSpec(memory_space=pltpu.HBM)] * len(operands),
        out_specs=[VMEM] * (len(kept) - 4),
        scratch_shapes=[
            pltpu.SMEM(lengths.shape, jnp.int32),
            *(pltpu.VMEM(a.shape, a.dtype) for a in held),
            pltpu.SemaphoreType.DMA((10,)),
            pltpu.SemaphoreType.DMA((len(kept) + 2 * gate.size // (rows_of(gate, line) * gate.shape[1]),)),
        ],
        compiler_params=params(12),
        name="attend",
    )(*operands)


def normed(rows, width):
    row_mean = jnp.sum(rows, axis=-1, keepdims=True) * (1.0 / width)
    row_var = jnp.sum(rows * rows, axis=-1, keepdims=True) * (1.0 / width) - row_mean * row_mean
    return (rows - row_mean) * lax.rsqrt(row_var + norm_eps)


def picking(shape, rule):
    row = lax.broadcasted_iota(jnp.int32, shape, 0)
    column = lax.broadcasted_iota(jnp.int32, shape, 1)
    return jnp.where(rule(row, column), 1.0, 0.0).astype(BF16)


def hidden_kernel(heads, gain, shift, copies):
    kept, width = heads.shape[1:]
    terms = heads[...].reshape(-1, width)
    rows = copies.shape[1]
    spread = terms.shape[0] // rows
    pick = picking(
        (rows, terms.shape[0]),
        lambda i, j: (i // kept == j // (kept * spread)) & (lax.rem(i, kept) == lax.rem(j, kept)),
    )
    rows = dot(pick, terms)
    hidden = (normed(rows, width) * gain[...] + shift[...]).astype(BF16)
    for i in range(copies.shape[0]):
        copies[i] = hidden


def hidden_copies(side, heads, gain, shift):
    kept, width = heads.shape[1:]
    return pl.pallas_call(
        hidden_kernel,
        out_shape=pltpu.VMEM((side, side * kept, width), BF16),
        in_specs=[VMEM] * 3,
        out_specs=VMEM,
        compiler_params=params(4),
        name="hidden_copies",
    )(*map(in_vmem, (heads, gain, shift)))


def halves(x):
    half = x.shape[1] // 2
    return x[:, :half], x[:, half:]


def branch_kernel(rows, gate_vector, mine, other, ids, shares, terms):
    x = rows[...]
    count, depth = x.shape
    tokens, line = ids.shape[1], lax.axis_size("ep_0")
    core = lax.axis_index("ep_2")
    chip = lax.axis_index("ep_0") * line + lax.axis_index("ep_1")
    row = lax.broadcasted_iota(jnp.int32, (count, tokens), 0)
    column = lax.broadcasted_iota(jnp.int32, (count, tokens), 1)
    outer, inner = row // (2 * line), (row // 2) % line
    far_z = jnp.where(core == 0, inner, outer)
    far_y = jnp.where(core == 0, outer, inner)
    match = column == 4 * (far_z * line + far_y) + 2 * core + (row & 1)
    lanes = gate_vector.shape[1]
    mixed = jnp.zeros((count, lanes), F32)
    for k in range(gate_vector.shape[0]):
        part = x[:, k * lanes : (k + 1) * lanes].astype(F32)
        mixed = mixed + part * gate_vector[k : k + 1].astype(F32)
    mixed = jnp.sum(mixed, axis=1, keepdims=True)
    mixing = 1.0 / (1.0 + jnp.exp(-mixed))
    split = 2 * EXPERT_UNITS
    units = []
    for pool, expert in ((mine, chip * 2 + core), (other, chip * 2 + 1 - core)):
        both = dot(x[:, :split], pool[:split, :split])
        for k in range(split, depth, split):
            both = both + dot(x[:, k : k + split], pool[:split, k : k + split])
        dense_both = dot_nt(x, pool[split + EXPERT_UNITS + DENSE_UNITS :])
        picked = jnp.where(ids[...] == expert, shares[...], 0.0)
        share_row = picked[0:1] + picked[1:2]
        share = jnp.sum(jnp.where(match, share_row, 0.0), axis=1, keepdims=True)
        a, b = halves(both)
        wide = (a / (1.0 + jnp.exp(-a)) * b * share).astype(BF16)
        a, b = halves(dense_both)
        narrow = (a / (1.0 + jnp.exp(-a)) * b * mixing).astype(BF16)
        units.append(jnp.concatenate([wide, narrow], axis=1))
    end = split + EXPERT_UNITS + DENSE_UNITS
    step = 512
    for k in range(0, depth, step):
        total = dot(units[0], mine[split:end, k : k + step])
        total = total + dot(units[1], other[split:end, k : k + step])
        terms[:, k : k + step] = total.astype(BF16)


def collect_kernel(terms, copies):
    total = terms[0].astype(F32)
    for i in range(1, terms.shape[0]):
        total = total + terms[i].astype(F32)
    total = total.astype(BF16).reshape(copies.shape[0], *copies.shape[2:])
    for i in range(copies.shape[1]):
        copies[:, i] = total


def branch_terms(*args):
    rows = args[0]
    return pl.pallas_call(
        branch_kernel,
        out_shape=pltpu.VMEM(rows.shape, BF16),
        in_specs=[VMEM] * len(args),
        out_specs=VMEM,
        compiler_params=params(8),
        cost_estimate=pl.CostEstimate(
            flops=2 * rows.size * 1024, bytes_accessed=4096, transcendentals=0
        ),
        name="branch_terms",
    )(*map(in_vmem, args))


def collected(count, terms):
    side, rows, width = terms.shape
    return pl.pallas_call(
        collect_kernel,
        out_shape=pltpu.VMEM((side, count, rows // side, width), BF16),
        in_specs=[VMEM],
        out_specs=VMEM,
        compiler_params=params(8),
        name="collected",
    )(in_vmem(terms))


def last_kernel(parts, hidden, gain, shift, out):
    kept = parts.shape[1]
    terms = parts[...].reshape(-1, parts.shape[2])
    core = lax.axis_index("ep_2")
    at = jnp.where(core == 0, lax.axis_index("ep_0"), lax.axis_index("ep_1"))
    pick = picking((kept, terms.shape[0]), lambda i, j: lax.rem(j, kept) == i)
    own = picking((kept, hidden.shape[1]), lambda i, j: j == at * kept + i)
    rows = alpha_scale * dot(own, hidden[0]) + dot(pick, terms)
    rows = normed(rows, rows.shape[1])
    width = out.shape[1]
    place = lax.axis_index("tp")
    own = rows[:, :width]
    for i in range(1, rows.shape[1] // width):
        own = jnp.where(place == i, rows[:, i * width : (i + 1) * width], own)
    out[...] = (own * gain[...] + shift[...]).astype(BF16)


def last_norm(parts, hidden, gain, shift):
    return pl.pallas_call(
        last_kernel,
        out_shape=jax.ShapeDtypeStruct((parts.shape[1], gain.shape[1]), BF16),
        in_specs=[VMEM] * 4,
        out_specs=VMEM,
        compiler_params=params(4),
        name="last_norm",
    )(*map(in_vmem, (parts, hidden, gain, shift)))


def lines(side, wide):
    z, y, c = (side * 2, 2, 1)
    alike = range(side)
    along_y = [[z * i + y * j for j in alike] for i in alike]
    along_z = [[z * i + y * j for i in alike] for j in alike]
    if wide:
        ways = range(wide)
        groups = along_z + [[g + c for g in group] for group in along_y]
        return [[g * wide + x for g in group for x in ways] for group in groups]
    return along_y + [[g + c for g in group] for group in along_z]


def along(array, side):
    return lax.all_to_all(array, EP, 0, 0, axis_index_groups=lines(side, 0), tiled=True)


def across(array, side, ways):
    groups = lines(side, ways)
    return lax.all_to_all(array, EP_TP, 0, 0, axis_index_groups=groups, tiled=True)


def per_device(
    tokens,
    w_query,
    w_key,
    w_value,
    w_forget,
    w_output,
    cache_keys,
    cache_values,
    cache_gates,
    lengths,
    ln1_gain,
    ln1_shift,
    gate_vector,
    dense_gate,
    dense_up,
    dense_down,
    expert_gate,
    expert_up,
    expert_down,
    expert_ids,
    expert_weights,
    ln2_gain,
    ln2_shift,
):
    kept = (
        expert_gate[0],
        expert_up[0],
        expert_down[0],
        dense_down,
        dense_gate.T,
        dense_up.T,
        gate_vector.reshape(-1, 128),
        expert_ids.T,
        expert_weights.T,
        ln1_gain[None],
        ln1_shift[None],
        ln2_gain[None],
        ln2_shift[None],
    )
    operands = (
        lengths,
        tokens,
        w_forget,
        cache_gates,
        w_query,
        w_key,
        w_value,
        w_output,
        cache_keys,
        cache_values,
    )
    side, ways = lax.axis_size("ep_0"), lax.axis_size("tp")
    heads, *kept = attend(side * ways, operands, kept)
    pool, vector, ids, shares, gain_1, shift_1, gain_2, shift_2 = kept
    other = lax.ppermute(pool, "ep_2", OTHER_CORE)
    copies = hidden_copies(side, across(heads, side, ways), gain_1, shift_1)
    rows = along(copies, side).reshape(-1, tokens.shape[1])
    terms = branch_terms(rows, vector, pool, other, ids, shares).reshape(copies.shape)
    sums = collected(ways, along(terms, side))
    parts = across(sums.reshape(-1, *sums.shape[2:]), side, ways)
    return last_norm(parts, copies, gain_2, shift_2)


def solution(mesh):
    torus = Mesh(mesh.devices.reshape(8, 8, 2, mesh.shape["tp"]), ("ep_0", "ep_1", "ep_2", "tp"))
    in_specs = (
        P(EP, None),
        P(None, "tp"),
        P(None, "tp"),
        P(None, "tp"),
        P("tp", None),
        P("tp", None),
        P(EP, "tp", None, None),
        P(EP, "tp", None, None),
        P(EP, "tp", None),
        P(EP),
        P(),
        P(),
        P(),
        P(None, EP_TP),
        P(None, EP_TP),
        P(EP_TP, None),
        P(EP, None, "tp"),
        P(EP, None, "tp"),
        P(EP, "tp", None),
        P(),
        P(),
        P("tp"),
        P("tp"),
    )
    out_specs = P(EP, "tp")
    return jax.shard_map(
        per_device, mesh=torus, in_specs=in_specs, out_specs=out_specs, check_vma=False
    )
```

```python
import functools

import jax
import jax.numpy as jnp
from jax import lax
from jax.experimental import pallas as pl
from jax.experimental.pallas import tpu as pltpu
from jax.sharding import Mesh
from jax.sharding import PartitionSpec as P

EP = ("ep_0", "ep_1", "ep_2")
EP_TP = ("ep_0", "ep_1", "ep_2", "tp")
OTHER_CORE = ((0, 1), (1, 0))

EXPERT_UNITS = 128
DENSE_UNITS = 16
alpha_scale = 1.4142135623730951
norm_eps = 1e-05

F32 = jnp.float32
BF16 = jnp.bfloat16
ANY = pl.BlockSpec(memory_space=pl.ANY)
VMEM = pl.BlockSpec(memory_space=pltpu.VMEM)
SMEM = pl.BlockSpec(memory_space=pltpu.SMEM)
NT = (((1,), (1,)), ((), ()))


def dot(a, b):
    return jnp.dot(a, b, preferred_element_type=F32)


def dot_nt(a, b):
    return lax.dot_general(a, b, NT, preferred_element_type=F32)


def in_vmem(x):
    return pltpu.with_memory_space_constraint(x, pltpu.VMEM)


def params(mib):
    return pltpu.CompilerParams(vmem_limit_bytes=mib << 20)


def attend_kernel(
    lengths_hbm,
    tokens_hbm,
    w_forget_hbm,
    cache_gates_hbm,
    w_query,
    w_key,
    w_value,
    w_output,
    cache_keys,
    cache_values,
    *rest,
):
    kept = (len(rest) - 8) // 2
    sources, (terms, *places) = rest[:kept], rest[kept : 2 * kept - 4]
    scratch = rest[2 * kept - 4 :]
    lengths, tokens, w_forget, cache_gates, q_v, k_v, v_v, o_v, keys_v, values_v, sems, kept_sems = scratch
    width = w_query.shape[1]
    moves = [
        pltpu.make_async_copy(src, dst, sems.at[i])
        for i, (src, dst) in enumerate(
            (
                (tokens_hbm, tokens),
                (w_forget_hbm, w_forget),
                (lengths_hbm, lengths),
                (cache_gates_hbm, cache_gates),
                (w_query, q_v),
                (cache_keys, keys_v),
                (w_key, k_v),
                (w_value, v_v),
                (cache_values, values_v),
                (w_output, o_v),
            )
        )
    ]
    targets = list(places)
    pool = places[0]
    gate, up, down, *dense = sources[:6]
    depth, width_up = pool.shape[1], gate.shape[1]
    rows = gate.shape[0] * 2 * width_up // depth
    pieces = []
    for k in range(gate.shape[0] // rows):
        for n, source in enumerate((gate, up)):
            start = (2 * k + n) * width_up
            pieces.append(
                (source.at[rows * k : rows * (k + 1)], pool.at[:rows, start : start + width_up])
            )
    for source in (down, *dense):
        pieces.append((source, pool.at[rows : rows + source.shape[0]]))
        rows += source.shape[0]
    pieces += zip(sources[6:], places[1:])
    kept_moves = [
        pltpu.make_async_copy(src, dst, kept_sems.at[i])
        for i, (src, dst) in enumerate(pieces)
    ]
    for move in moves:
        move.start()

    for move in moves[:4]:
        move.wait()
    x = tokens[...]
    scale = width ** (-0.5)
    length = cache_gates.shape[2]
    forget = jnp.sum(x.astype(F32) * w_forget[...].astype(F32), axis=1, keepdims=True)
    forget_new = jax.nn.log_sigmoid(forget)
    second = lax.broadcasted_iota(jnp.int32, (2, 1), 0) == 1
    used = jnp.where(second, lengths[1], lengths[0])
    gates = jnp.where(second, cache_gates[1], cache_gates[0])
    positions = lax.broadcasted_iota(jnp.int32, (2, length), 1)
    last_gate = jnp.sum(jnp.where(positions == used - 1, gates, 0.0), axis=1, keepdims=True)
    decay_bias = (last_gate + forget_new) - gates

    moves[4].wait()
    for move in kept_moves:
        move.start()
    query = dot(x, q_v[...]).astype(BF16)
    moves[5].wait()
    scores = jnp.where(second, dot_nt(query, keys_v[1, 0]), dot_nt(query, keys_v[0, 0])) * scale
    scores = jnp.where(positions < used, scores + decay_bias, -jnp.inf)
    moves[6].wait()
    moves[7].wait()
    new_key = dot(x, k_v[...]).astype(BF16)
    new_value = dot(x, v_v[...]).astype(BF16)
    own_score = (
        jnp.sum(query.astype(F32) * new_key.astype(F32), axis=1, keepdims=True) * scale
    )
    peak = jnp.maximum(jnp.max(scores, axis=1, keepdims=True), own_score)
    exp_terms = jnp.exp(scores - peak)
    own_exp = jnp.exp(own_score - peak)
    denominator = jnp.sum(exp_terms, axis=1, keepdims=True) + own_exp
    probs = (exp_terms / denominator).astype(BF16)
    own_prob = (own_exp / denominator).astype(BF16)
    moves[8].wait()
    weighted = jnp.where(second, dot(probs, values_v[1, 0]), dot(probs, values_v[0, 0]))
    weighted = weighted + own_prob.astype(F32) * new_value.astype(F32)
    moves[9].wait()
    term = dot(weighted.astype(BF16), o_v[...])
    term = (term + (alpha_scale / lax.axis_size("tp")) * x.astype(F32)).astype(BF16)
    for i in range(terms.shape[0]):
        terms[i] = term
    for move in kept_moves:
        move.wait()


def rows_of(gate, line):
    return 2 * gate.size // line


def attend(copies, operands, kept):
    operands = [pltpu.with_memory_space_constraint(a, pltpu.HBM) for a in (*operands, *kept)]
    lengths, tokens, w_forget, gates, w_query, w_key, w_value, w_output, keys, values = operands[:10]
    gate, up, down, *dense = kept[:6]
    line = down.shape[1]
    rows = (gate.size + up.size) // line + down.shape[0] + sum(a.shape[0] for a in dense)
    held = (tokens, w_forget, gates, w_query, w_key, w_value, w_output, keys, values)
    return pl.pallas_call(
        attend_kernel,
        out_shape=[pltpu.VMEM((copies, tokens.shape[0], w_output.shape[1]), BF16)]
        + [pltpu.VMEM((rows, line), BF16)]
        + [pltpu.VMEM(a.shape, a.dtype) for a in kept[6:]],
        in_specs=[pl.BlockSpec(memory_space=pltpu.HBM)] * len(operands),
        out_specs=[VMEM] * (len(kept) - 4),
        scratch_shapes=[
            pltpu.SMEM(lengths.shape, jnp.int32),
            *(pltpu.VMEM(a.shape, a.dtype) for a in held),
            pltpu.SemaphoreType.DMA((10,)),
            pltpu.SemaphoreType.DMA((len(kept) + 2 * gate.size // (rows_of(gate, line) * gate.shape[1]),)),
        ],
        compiler_params=params(12),
        name="attend",
    )(*operands)


def normed(rows, width):
    row_mean = jnp.sum(rows, axis=-1, keepdims=True) * (1.0 / width)
    row_var = jnp.sum(rows * rows, axis=-1, keepdims=True) * (1.0 / width) - row_mean * row_mean
    return (rows - row_mean) * lax.rsqrt(row_var + norm_eps)


def picking(shape, rule):
    row = lax.broadcasted_iota(jnp.int32, shape, 0)
    column = lax.broadcasted_iota(jnp.int32, shape, 1)
    return jnp.where(rule(row, column), 1.0, 0.0).astype(BF16)


def hidden_kernel(heads, gain, shift, copies):
    kept, width = heads.shape[1:]
    terms = heads[...].reshape(-1, width)
    rows = copies.shape[1]
    spread = terms.shape[0] // rows
    pick = picking(
        (rows, terms.shape[0]),
        lambda i, j: (i // kept == j // (kept * spread)) & (lax.rem(i, kept) == lax.rem(j, kept)),
    )
    rows = dot(pick, terms)
    hidden = (normed(rows, width) * gain[...] + shift[...]).astype(BF16)
    for i in range(copies.shape[0]):
        copies[i] = hidden


def hidden_copies(side, heads, gain, shift):
    kept, width = heads.shape[1:]
    return pl.pallas_call(
        hidden_kernel,
        out_shape=pltpu.VMEM((side, side * kept, width), BF16),
        in_specs=[VMEM] * 3,
        out_specs=VMEM,
        compiler_params=params(4),
        name="hidden_copies",
    )(*map(in_vmem, (heads, gain, shift)))


def halves(x):
    half = x.shape[1] // 2
    return x[:, :half], x[:, half:]


def branch_kernel(rows, gate_vector, mine, other, ids, shares, terms):
    x = rows[...]
    count, depth = x.shape
    tokens, line = ids.shape[1], lax.axis_size("ep_0")
    core = lax.axis_index("ep_2")
    chip = lax.axis_index("ep_0") * line + lax.axis_index("ep_1")
    row = lax.broadcasted_iota(jnp.int32, (count, tokens), 0)
    column = lax.broadcasted_iota(jnp.int32, (count, tokens), 1)
    outer, inner = row // (2 * line), (row // 2) % line
    far_z = jnp.where(core == 0, inner, outer)
    far_y = jnp.where(core == 0, outer, inner)
    match = column == 4 * (far_z * line + far_y) + 2 * core + (row & 1)
    lanes = gate_vector.shape[1]
    mixed = jnp.zeros((count, lanes), F32)
    for k in range(gate_vector.shape[0]):
        part = x[:, k * lanes : (k + 1) * lanes].astype(F32)
        mixed = mixed + part * gate_vector[k : k + 1].astype(F32)
    mixed = jnp.sum(mixed, axis=1, keepdims=True)
    mixing = 1.0 / (1.0 + jnp.exp(-mixed))
    split = 2 * EXPERT_UNITS
    units = []
    for pool, expert in ((mine, chip * 2 + core), (other, chip * 2 + 1 - core)):
        both = dot(x[:, :split], pool[:split, :split])
        for k in range(split, depth, split):
            both = both + dot(x[:, k : k + split], pool[:split, k : k + split])
        dense_both = dot_nt(x, pool[split + EXPERT_UNITS + DENSE_UNITS :])
        picked = jnp.where(ids[...] == expert, shares[...], 0.0)
        share_row = picked[0:1] + picked[1:2]
        share = jnp.sum(jnp.where(match, share_row, 0.0), axis=1, keepdims=True)
        a, b = halves(both)
        wide = (a / (1.0 + jnp.exp(-a)) * b * share).astype(BF16)
        a, b = halves(dense_both)
        narrow = (a / (1.0 + jnp.exp(-a)) * b * mixing).astype(BF16)
        units.append(jnp.concatenate([wide, narrow], axis=1))
    end = split + EXPERT_UNITS + DENSE_UNITS
    step = 512
    for k in range(0, depth, step):
        total = dot(units[0], mine[split:end, k : k + step])
        total = total + dot(units[1], other[split:end, k : k + step])
        terms[:, k : k + step] = total.astype(BF16)


def collect_kernel(terms, copies):
    total = terms[0].astype(F32)
    for i in range(1, terms.shape[0]):
        total = total + terms[i].astype(F32)
    total = total.astype(BF16).reshape(copies.shape[0], *copies.shape[2:])
    for i in range(copies.shape[1]):
        copies[:, i] = total


def branch_terms(*args):
    rows = args[0]
    return pl.pallas_call(
        branch_kernel,
        out_shape=pltpu.VMEM(rows.shape, BF16),
        in_specs=[VMEM] * len(args),
        out_specs=VMEM,
        compiler_params=params(8),
        cost_estimate=pl.CostEstimate(
            flops=2 * rows.size * 1024, bytes_accessed=4096, transcendentals=0
        ),
        name="branch_terms",
    )(*map(in_vmem, args))


def collected(count, terms):
    side, rows, width = terms.shape
    return pl.pallas_call(
        collect_kernel,
        out_shape=pltpu.VMEM((side, count, rows // side, width), BF16),
        in_specs=[VMEM],
        out_specs=VMEM,
        compiler_params=params(8),
        name="collected",
    )(in_vmem(terms))


def last_kernel(parts, hidden, gain, shift, out):
    kept = parts.shape[1]
    terms = parts[...].reshape(-1, parts.shape[2])
    core = lax.axis_index("ep_2")
    at = jnp.where(core == 0, lax.axis_index("ep_0"), lax.axis_index("ep_1"))
    pick = picking((kept, terms.shape[0]), lambda i, j: lax.rem(j, kept) == i)
    own = picking((kept, hidden.shape[1]), lambda i, j: j == at * kept + i)
    rows = alpha_scale * dot(own, hidden[0]) + dot(pick, terms)
    rows = normed(rows, rows.shape[1])
    width = out.shape[1]
    place = lax.axis_index("tp")
    own = rows[:, :width]
    for i in range(1, rows.shape[1] // width):
        own = jnp.where(place == i, rows[:, i * width : (i + 1) * width], own)
    out[...] = (own * gain[...] + shift[...]).astype(BF16)


def last_norm(parts, hidden, gain, shift):
    return pl.pallas_call(
        last_kernel,
        out_shape=jax.ShapeDtypeStruct((parts.shape[1], gain.shape[1]), BF16),
        in_specs=[VMEM] * 4,
        out_specs=VMEM,
        compiler_params=params(4),
        name="last_norm",
    )(*map(in_vmem, (parts, hidden, gain, shift)))


def lines(side, wide):
    z, y, c = (side * 2, 2, 1)
    alike = range(side)
    along_y = [[z * i + y * j for j in alike] for i in alike]
    along_z = [[z * i + y * j for i in alike] for j in alike]
    if wide:
        ways = range(wide)
        groups = along_z + [[g + c for g in group] for group in along_y]
        return [[g * wide + x for g in group for x in ways] for group in groups]
    return along_y + [[g + c for g in group] for group in along_z]


def along(array, side):
    return lax.all_to_all(array, EP, 0, 0, axis_index_groups=lines(side, 0), tiled=True)


def across(array, side, ways):
    groups = lines(side, ways)
    return lax.all_to_all(array, EP_TP, 0, 0, axis_index_groups=groups, tiled=True)


def per_device(
    tokens,
    w_query,
    w_key,
    w_value,
    w_forget,
    w_output,
    cache_keys,
    cache_values,
    cache_gates,
    lengths,
    ln1_gain,
    ln1_shift,
    gate_vector,
    dense_gate,
    dense_up,
    dense_down,
    expert_gate,
    expert_up,
    expert_down,
    expert_ids,
    expert_weights,
    ln2_gain,
    ln2_shift,
):
    kept = (
        expert_gate[0],
        expert_up[0],
        expert_down[0],
        dense_down,
        dense_gate.T,
        dense_up.T,
        gate_vector.reshape(-1, 128),
        expert_ids.T,
        expert_weights.T,
        ln1_gain[None],
        ln1_shift[None],
        ln2_gain[None],
        ln2_shift[None],
    )
    operands = (
        lengths,
        tokens,
        w_forget,
        cache_gates,
        w_query,
        w_key,
        w_value,
        w_output,
        cache_keys,
        cache_values,
    )
    side, ways = lax.axis_size("ep_0"), lax.axis_size("tp")
    heads, *kept = attend(side * ways, operands, kept)
    pool, vector, ids, shares, gain_1, shift_1, gain_2, shift_2 = kept
    other = lax.ppermute(pool, "ep_2", OTHER_CORE)
    copies = hidden_copies(side, across(heads, side, ways), gain_1, shift_1)
    rows = along(copies, side).reshape(-1, tokens.shape[1])
    terms = branch_terms(rows, vector, pool, other, ids, shares).reshape(copies.shape)
    sums = collected(ways, along(terms, side))
    parts = across(sums.reshape(-1, *sums.shape[2:]), side, ways)
    return last_norm(parts, copies, gain_2, shift_2)


def solution(mesh):
    torus = Mesh(mesh.devices.reshape(8, 8, 2, mesh.shape["tp"]), ("ep_0", "ep_1", "ep_2", "tp"))
    in_specs = (
        P(EP, None),
        P(None, "tp"),
        P(None, "tp"),
        P(None, "tp"),
        P("tp", None),
        P("tp", None),
        P(EP, "tp", None, None),
        P(EP, "tp", None, None),
        P(EP, "tp", None),
        P(EP),
        P(),
        P(),
        P(),
        P(None, EP_TP),
        P(None, EP_TP),
        P(EP_TP, None),
        P(EP, None, "tp"),
        P(EP, None, "tp"),
        P(EP, "tp", None),
        P(),
        P(),
        P("tp"),
        P("tp"),
    )
    out_specs = P(EP, "tp")
    return jax.shard_map(
        per_device, mesh=torus, in_specs=in_specs, out_specs=out_specs, check_vma=False
    )
```
